32 devices in a mesh: sp: 8 (over z, y), tp: 4 (over x, core).
Axes of the slice: x: 2, y: 2, z: 4, core: 2. Of those that a mesh axis runs over, the one named last changes fastest.
Arguments:
- residual_in: bfloat16 [4096, 2048], P('sp'), may hold values from -6 to 6
- queries_nope: bfloat16 [4096, 1024], P('sp', 'tp'), may hold values from -15 to 15
- queries_rope: bfloat16 [4096, 512], P('sp', 'tp'), may hold values from -400 to 400
- latents: bfloat16 [4096, 256], P('sp'), may hold values from -6 to 6
- rope_keys: bfloat16 [4096, 32], P('sp'), may hold values from -8 to 8
- latent_norm_gain: float32 [256], replicated, may hold values from 0.1 to 1.9
- key_up_weight: bfloat16 [256, 1024], P(None, 'tp'), may hold values from -0.375 to 0.375
- value_up_weight: bfloat16 [256, 1024], P(None, 'tp'), may hold values from -0.375 to 0.375
- w_out: bfloat16 [1024, 2048], P('tp'), may hold values from -0.59765625 to 0.59765625
- norm_gain: float32 [2048], replicated, may hold values from 0.1 to 1.9
- w_up: bfloat16 [2048, 8192], P('sp', 'tp'), may hold values from -0.125 to 0.125
- w_down: bfloat16 [8192, 2048], P('tp', 'sp'), may hold values from -0.0625 to 0.0625
Outputs:
- layer_out: bfloat16 [4096, 2048], P('sp', 'tp')
The draws below stay inside these ranges and needn't reach their ends.
All inputs are finite; a program needn't handle non-finite values.
Results may differ from the reference program's by a relative error of at most 0.015.
Values may be sent and summed in bfloat16 or wider, within the bound.
A program may use at most 128 MiB of HBM per device.

```python
import math
import jax
import jax.numpy as jnp
from jax import lax

D = 2048
HEAD_TOTAL = 16
UNROTATED_WIDTH = 64
ROPE = 32
VALUE_WIDTH = 64
LATENT_WIDTH = 256
FF = 8192
TOKEN_TOTAL = 4096
N_TP = 4


def shared_rope(key):
    base_rows = jnp.clip(jax.random.normal(jax.random.fold_in(key, 11), (TOKEN_TOTAL, ROPE), jnp.float32), -4.0, 4.0)
    return base_rows


def draw_rope_keys(key, part):
    base_rows = shared_rope(key)
    return base_rows.astype(jnp.bfloat16)


def draw_queries_rope(key, part):
    drawn = jnp.clip(jax.random.normal(jax.random.fold_in(key, 21), (TOKEN_TOTAL, HEAD_TOTAL * ROPE), jnp.float32) * 2.5, -15.0, 15.0)
    return drawn.astype(jnp.bfloat16)


def level_of(stream_key, dims, shards, least, largest):
    factor_of, own = 1.0, jax.random.fold_in(stream_key, 6)
    for axis_at, blocks in shards:
        draws = jnp.exp(jax.random.uniform(jax.random.fold_in(own, axis_at), (blocks,), jnp.float32, least / len(shards), largest / len(shards)))
        factor_of = factor_of * jnp.repeat(draws, dims[axis_at] // blocks).reshape([-1 if axis == axis_at else 1 for axis in range(len(dims))])
    return factor_of


def bell_draw(own_key, extent, scale, reach, pieces=(), kind=jnp.bfloat16):
    gain = level_of(own_key, extent, pieces, -0.22, 0.18) if pieces else 1.0
    entries = jax.random.normal(own_key, extent, jnp.float32) * scale * gain
    return jnp.minimum(jnp.maximum(entries, -reach), reach).astype(kind)


def setup_inputs(seed: int = 0) -> dict:
    keys = jax.random.split(jax.random.key(seed), 13)
    residual_in = bell_draw(keys[0], (TOKEN_TOTAL, D), 1.0, 6.0, ((0, 8),))
    queries_nope = bell_draw(keys[1], (TOKEN_TOTAL, HEAD_TOTAL * UNROTATED_WIDTH), 2.5, 15.0, ((0, 8), (1, 4)))
    queries_rope = draw_queries_rope(jax.random.fold_in(keys[12], 71), 0)
    latents = bell_draw(keys[3], (TOKEN_TOTAL, LATENT_WIDTH), 1.0, 6.0, ((0, 8),))
    rope_keys = draw_rope_keys(jax.random.fold_in(keys[12], 71), 0)
    latent_norm_gain = jnp.clip(1.0 + 0.18 * jax.random.normal(keys[5], (LATENT_WIDTH,), jnp.float32), 0.1, 1.9)
    key_up_weight = bell_draw(keys[6], (LATENT_WIDTH, HEAD_TOTAL * UNROTATED_WIDTH), LATENT_WIDTH ** -0.5, 0.375, ((1, 4),))
    value_up_weight = bell_draw(keys[7], (LATENT_WIDTH, HEAD_TOTAL * VALUE_WIDTH), LATENT_WIDTH ** -0.5, 0.375, ((1, 4),))
    w_out = bell_draw(keys[8], (HEAD_TOTAL * VALUE_WIDTH, D), 0.1, 0.59765625, ((0, 4),))
    norm_gain = jnp.clip(1.0 + 0.18 * jax.random.normal(keys[9], (D,), jnp.float32), 0.1, 1.9)
    w_up = bell_draw(keys[10], (D, FF), D ** -0.5, 0.125, ((0, 8), (1, 4)))
    w_down = bell_draw(keys[11], (FF, D), FF ** -0.5, 0.0625, ((0, 4), (1, 8)))
    return dict(residual_in=residual_in, queries_nope=queries_nope, queries_rope=queries_rope, latents=latents, rope_keys=rope_keys, latent_norm_gain=latent_norm_gain, key_up_weight=key_up_weight, value_up_weight=value_up_weight, w_out=w_out, norm_gain=norm_gain, w_up=w_up, w_down=w_down)


rope_base = 10000.0
epsilon = 1e-06

def rotate(vectors, phases):
    half_width = vectors.shape[-1] // 2
    first_half = vectors[..., :half_width]
    second_half = vectors[..., half_width:]
    cosine = jnp.cos(phases)
    sine = jnp.sin(phases)
    return jnp.concatenate([first_half * cosine - second_half * sine, second_half * cosine + first_half * sine], axis=-1)

def rope_phases(positions, width):
    inverse = 1.0 / rope_base ** (jnp.arange(0, width, 2, dtype=jnp.float32) / width)
    return positions.astype(jnp.float32)[:, None] * inverse[None, :]

def rms_scale(vectors, gain_vec):
    return vectors * lax.rsqrt(lax.optimization_barrier(jnp.mean(vectors * vectors, axis=-1, keepdims=True)) + epsilon) * gain_vec.astype(jnp.float32)

def reference(residual_in, queries_nope, queries_rope, latents, rope_keys, latent_norm_gain, key_up_weight, value_up_weight, w_out, norm_gain, w_up, w_down):
    positions = jnp.arange(TOKEN_TOTAL, dtype=jnp.int32)
    phases = rope_phases(positions, ROPE)
    q_rot = rotate(queries_rope.astype(jnp.float32).reshape(TOKEN_TOTAL, HEAD_TOTAL, ROPE), phases[:, None, :]).astype(jnp.bfloat16)
    queries = jnp.concatenate([queries_nope.reshape(TOKEN_TOTAL, HEAD_TOTAL, UNROTATED_WIDTH), q_rot], axis=2)
    lat_norm = rms_scale(latents.astype(jnp.float32), latent_norm_gain).astype(jnp.bfloat16)
    key_nope = jnp.dot(lat_norm, key_up_weight, preferred_element_type=jnp.float32).astype(jnp.bfloat16).reshape(TOKEN_TOTAL, HEAD_TOTAL, UNROTATED_WIDTH)
    values = jnp.dot(lat_norm, value_up_weight, preferred_element_type=jnp.float32).astype(jnp.bfloat16).reshape(TOKEN_TOTAL, HEAD_TOTAL, VALUE_WIDTH)
    key_rot = rotate(rope_keys.astype(jnp.float32), phases).astype(jnp.bfloat16)
    key_all = jnp.concatenate([key_nope, jnp.broadcast_to(key_rot[:, None, :], (TOKEN_TOTAL, HEAD_TOTAL, ROPE))], axis=2).astype(jnp.float32)
    value_all = values.astype(jnp.float32)
    score_scale = 1.0 / math.sqrt(UNROTATED_WIDTH + ROPE)
    query_rows = math.gcd(TOKEN_TOTAL, 128)

    def attend(query_block):
        scores = jnp.einsum('qhd,khd->hqk', query_block.astype(jnp.float32), key_all) * score_scale
        row_peak = lax.optimization_barrier(jnp.max(scores, axis=2, keepdims=True))
        weights = jnp.exp(scores - row_peak)
        denominator = lax.optimization_barrier(jnp.sum(weights, axis=2))
        rounded = lax.optimization_barrier(weights.astype(jnp.bfloat16)).astype(jnp.float32)
        weighted = jnp.einsum('hqk,khd->qhd', rounded, value_all)
        return (weighted / jnp.transpose(denominator)[:, :, None]).astype(jnp.bfloat16)
    attended = lax.map(attend, queries.reshape(TOKEN_TOTAL // query_rows, query_rows, HEAD_TOTAL, UNROTATED_WIDTH + ROPE))
    attended = attended.reshape(TOKEN_TOTAL, HEAD_TOTAL * VALUE_WIDTH)
    group_cols = HEAD_TOTAL * VALUE_WIDTH // N_TP
    summed = jnp.zeros((TOKEN_TOTAL, D), jnp.float32)
    for member in range(N_TP):
        part_term = jnp.dot(attended[:, member * group_cols:(member + 1) * group_cols], w_out[member * group_cols:(member + 1) * group_cols], preferred_element_type=jnp.float32)
        summed = summed + lax.optimization_barrier(part_term.astype(jnp.bfloat16)).astype(jnp.float32)
    stream = residual_in.astype(jnp.float32) + summed
    normed = rms_scale(stream, norm_gain).astype(jnp.bfloat16)
    upward = jnp.dot(normed, w_up, preferred_element_type=jnp.float32)
    hidden = jnp.square(jax.nn.relu(upward)).astype(jnp.bfloat16)
    group_units = FF // N_TP
    mixer = jnp.zeros((TOKEN_TOTAL, D), jnp.float32)
    for member in range(N_TP):
        part_term = jnp.dot(hidden[:, member * group_units:(member + 1) * group_units], w_down[member * group_units:(member + 1) * group_units], preferred_element_type=jnp.float32)
        mixer = mixer + lax.optimization_barrier(part_term.astype(jnp.bfloat16)).astype(jnp.float32)
    return (stream + mixer).astype(jnp.bfloat16)
```

```python
import functools
import math

import jax
import jax.numpy as jnp
from jax import lax
from jax.experimental import pallas as pl
from jax.experimental.pallas import tpu as pltpu
from jax.sharding import PartitionSpec as P

UNROTATED_WIDTH = 64
ROPE = 32
LANES = 128
CHUNKS = 4
CUTS = 2

rope_base = 10000.0
epsilon = 1e-06
F32 = jnp.float32
BF16 = jnp.bfloat16
MESH = pl.DeviceIdType.MESH
NT = (((1,), (1,)), ((), ()))


def rotate(vectors, phases):
    half_width = vectors.shape[-1] // 2
    first_half = vectors[..., :half_width]
    second_half = vectors[..., half_width:]
    cosine = jnp.cos(phases)
    sine = jnp.sin(phases)
    return jnp.concatenate(
        [first_half * cosine - second_half * sine, second_half * cosine + first_half * sine],
        axis=-1,
    )


def rope_phases(positions, width):
    inverse = 1.0 / rope_base ** (jnp.arange(0, width, 2, dtype=jnp.float32) / width)
    return positions.astype(jnp.float32)[:, None] * inverse[None, :]


def rms_scale(vectors, gain_vec):
    return (
        vectors
        * lax.rsqrt(jnp.mean(vectors * vectors, axis=-1, keepdims=True) + epsilon)
        * gain_vec
    )


def ring_of(index, n):
    return index // 2 + (index % 2) * (n - 1 - 2 * (index // 2))


def index_of(place, n):
    return 2 * place + (place // (n // 2)) * (2 * n - 1 - 4 * place)


def ring_ids(n):
    place = ring_of(lax.axis_index("sp"), n)

    def at(offset):
        return index_of((place + offset + 2 * n) % n, n)

    return at


def attention_kernel(
    n, n_tp, heads, scale, q_ref, x_ref, wk_in, wv_in, wo_ref, wu_ref,
    part_ref, full_ref,
    wk_ref, wv_ref, xs, peak, acc, xsend, xrecv, ssend, srecv, wsend, wrecv, own_sem,
):
    at = ring_ids(n)
    tp = lax.axis_index("tp")
    me = lax.axis_index("sp")
    to = ((at(1), tp), (at(-1), tp))
    peers = [(tp + k) % n_tp for k in range(1, n_tp)]
    onward = (at(1 - 2 * (tp % 2)), tp)
    barrier = pltpu.get_barrier_semaphore()
    for target in list(to) + [(me, p) for p in peers]:
        pl.semaphore_signal(barrier, inc=1, device_id=target, device_id_type=MESH)
    pl.semaphore_wait(barrier, 2 + n_tp - 1)

    latent = wk_ref.shape[1]
    value_width = wv_ref.shape[0] // heads

    def x_copy(step, src):
        return pltpu.make_async_remote_copy(
            src_ref=src, dst_ref=xs.at[step + 1, tp],
            send_sem=xsend.at[step], recv_sem=xrecv.at[step],
            device_id=onward, device_id_type=MESH,
        )

    def share(step, k):
        return pltpu.make_async_remote_copy(
            src_ref=xs.at[step, tp], dst_ref=xs.at[step, tp],
            send_sem=ssend.at[step, k], recv_sem=srecv.at[step, k],
            device_id=(me, peers[k]), device_id_type=MESH,
        )

    def share_wait(step):
        for k in range(n_tp - 1):
            pltpu.make_async_remote_copy(
                src_ref=xs.at[step, tp], dst_ref=xs.at[step, (tp + n_tp - 1 - k) % n_tp],
                send_sem=ssend.at[step, k], recv_sem=srecv.at[step, k],
                device_id=(me, peers[k]), device_id_type=MESH,
            ).wait_recv()

    def w_copy(step, half, c, first):
        owner = at(-step) if half == 0 else at(step)
        return pltpu.make_async_remote_copy(
            src_ref=wu_ref.at[half, c] if first else full_ref.at[owner, half, c],
            dst_ref=full_ref.at[owner, half, c],
            send_sem=wsend.at[step, half, c], recv_sem=wrecv.at[step, half, c],
            device_id=to[half], device_id_type=MESH,
        )

    x_copy(0, x_ref.at[tp]).start()
    for c in range(CHUNKS):
        for half in range(2):
            w_copy(0, half, c, True).start()
    own = pltpu.make_async_copy(wu_ref, full_ref.at[me], own_sem)
    own.start()
    wk_ref[...] = jnp.transpose(wk_in[...].astype(F32)).astype(BF16)
    wv_ref[...] = jnp.transpose(wv_in[...].astype(F32)).astype(BF16)
    peak[...] = jnp.full(peak.shape, -1e30, F32)
    acc[...] = jnp.zeros(acc.shape, F32)

    def attend(blocks):
        block = jnp.concatenate(blocks, axis=1)
        lat = block[:latent]
        rot = block[latent:]
        keys = block.shape[1]
        k_all = jnp.dot(wk_ref[...], lat, preferred_element_type=F32).astype(BF16)
        v_all = jnp.dot(wv_ref[...], lat, preferred_element_type=F32).astype(BF16)
        k_pad = jnp.zeros((LANES - UNROTATED_WIDTH - rot.shape[0], keys), BF16)
        ones = jnp.ones((16, keys), BF16)
        v_pad = jnp.zeros((LANES - value_width - 16, keys), BF16)
        for h in range(heads):
            k_h = jnp.concatenate(
                [k_all[h * UNROTATED_WIDTH:(h + 1) * UNROTATED_WIDTH], rot, k_pad], axis=0)
            v_h = jnp.concatenate(
                [v_all[h * value_width:(h + 1) * value_width], ones, v_pad], axis=0)
            s = jnp.dot(q_ref[:, h * LANES:(h + 1) * LANES], k_h, preferred_element_type=F32)
            old = peak[h]
            new = jnp.maximum(old, jnp.max(s, axis=1, keepdims=True))
            p = jnp.exp2((s - new) * scale).astype(BF16)
            acc[h] = acc[h] * jnp.exp2((old - new) * scale) + lax.dot_general(
                p, v_h, NT, preferred_element_type=F32)
            peak[h] = new

    def turn(i, carry):
        x_copy(i - 1, x_ref.at[tp]).wait_recv()
        x_copy(i, xs.at[i, tp]).start()
        for k in range(n_tp - 1):
            share(i, k).start()
        for c in range(CHUNKS):
            for half in range(2):
                w_copy(i - 1, half, c, True).wait_recv()
                w_copy(i, half, c, False).start()

        @pl.when(i > 1)
        def _():
            share_wait(i - 1)
            attend([xs[i - 1, t] for t in range(n_tp)])

        return carry

    attend([x_ref[t] for t in range(n_tp)])
    lax.fori_loop(1, n - 1, turn, 0)
    x_copy(n - 2, x_ref.at[tp]).wait_recv()
    for k in range(n_tp - 1):
        share(n - 1, k).start()

    def last(i, carry):
        share_wait(i)
        attend([xs[i, t] for t in range(n_tp)])
        return carry

    lax.fori_loop(n - 2, n, last, 0)

    width = part_ref.shape[2]
    group = []
    for h in range(heads):
        a = acc[h]
        group.append((a[:, :value_width] / a[:, value_width:value_width + 1]).astype(BF16))
    attended = jnp.concatenate(group, axis=1)
    for j in range(part_ref.shape[0]):
        part_ref[j] = jnp.dot(
            attended, wo_ref[:, j * width:(j + 1) * width], preferred_element_type=F32
        ).astype(BF16)

    own.wait()
    for c in range(CHUNKS):
        for half in range(2):
            w_copy(n - 2, half, c, True).wait_recv()

    def drain(i, carry):
        x_copy(i, x_ref.at[tp]).wait_send()
        for k in range(n_tp - 1):
            share(i + 1, k).wait_send()
        for c in range(CHUNKS):
            for half in range(2):
                w_copy(i, half, c, True).wait_send()
        return carry

    lax.fori_loop(0, n - 1, drain, 0)


def feed_kernel(
    n, n_tp, narrow, part_ref, res_hbm, gain_ref, up_hbm, wd_hbm,
    out_ref,
    res_ref, up, down, parts, ys, sq, own_stream, hidden, pieces, fin,
    dsend, drecv, psend, precv, ysend, yrecv, qsend, qrecv, fsend, frecv, local,
):
    at = ring_ids(n)
    tp = lax.axis_index("tp")
    sp = lax.axis_index("sp")
    to = ((at(1), tp), (at(-1), tp))
    peers = [(tp + k) % n_tp for k in range(1, n_tp)]
    barrier = pltpu.get_barrier_semaphore()
    for target in list(to) + [(sp, p) for p in peers]:
        pl.semaphore_signal(barrier, inc=1, device_id=target, device_id_type=MESH)
    pl.semaphore_wait(barrier, 2 + n_tp - 1)

    rows, width = res_ref.shape
    per = n // n_tp

    lines = down.shape[2] // CHUNKS

    def own_half(half):
        if narrow:
            return wd_hbm.at[half]
        return wd_hbm.at[:, half * down.shape[3]:(half + 1) * down.shape[3]]

    def d_copy(step, half, c, first):
        span = pl.ds(c * lines, lines)
        if not first:
            src = down.at[step, half, span]
        elif narrow:
            src = wd_hbm.at[half, span]
        else:
            src = wd_hbm.at[span, half * down.shape[3]:(half + 1) * down.shape[3]]
        return pltpu.make_async_remote_copy(
            src_ref=src, dst_ref=down.at[step + 1, half, span],
            send_sem=dsend.at[step, half, c], recv_sem=drecv.at[step, half, c],
            device_id=to[half], device_id_type=MESH,
        )

    def p_copy(k):
        peer = peers[k]
        return pltpu.make_async_remote_copy(
            src_ref=part_ref.at[peer], dst_ref=parts.at[k],
            send_sem=psend.at[k], recv_sem=precv.at[k],
            device_id=(sp, peer), device_id_type=MESH,
        )

    def y_copy(k):
        return pltpu.make_async_remote_copy(
            src_ref=ys.at[tp], dst_ref=ys.at[tp],
            send_sem=ysend.at[k], recv_sem=yrecv.at[k],
            device_id=(sp, peers[k]), device_id_type=MESH,
        )

    def q_copy(k):
        return pltpu.make_async_remote_copy(
            src_ref=sq.at[0], dst_ref=sq.at[k + 1],
            send_sem=qsend.at[k], recv_sem=qrecv.at[k],
            device_id=(sp, peers[k]), device_id_type=MESH,
        )

    def landed(step, c):
        for half in range(2):
            d_copy(step, half, c, True).wait_recv()

    def event(step, c):
        landed(step - 1, c)
        for half in range(2):
            d_copy(step, half, c, False).start()

    def events(first, last):
        for tick in range(first, last):
            event(1 + tick // CHUNKS, tick % CHUNKS)

    for c in range(CHUNKS):
        for half in range(2):
            d_copy(0, half, c, True).start()
    for k in range(n_tp - 1):
        p_copy(k).start()
    loads = [
        pltpu.make_async_copy(
            res_hbm.at[:, pl.ds(pl.multiple_of(tp * width, LANES), width)], res_ref, local.at[0]),
        pltpu.make_async_copy(up_hbm, up, local.at[1]),
        pltpu.make_async_copy(own_half(0), down.at[0, 0], local.at[2]),
        pltpu.make_async_copy(own_half(1), down.at[0, 1], local.at[3]),
    ]
    for load in loads:
        load.start()

    early = 4
    events(0, 6)
    for k in range(n_tp - 1):
        p_copy(k).wait_recv()
    loads[0].wait()
    stream = part_ref[tp].astype(F32)
    for k in range(n_tp - 1):
        stream = stream + parts[k].astype(F32)
    stream = stream + res_ref[...].astype(F32)
    own_stream[...] = stream
    ys[tp] = (stream * gain_ref[tp]).astype(BF16)
    total = jnp.sum(stream * stream, axis=1, keepdims=True)
    sq[0] = jnp.transpose(jnp.broadcast_to(total, (rows, LANES)))[:8]
    for k in range(n_tp - 1):
        q_copy(k).start()
        y_copy(k).start()
    events(6, 12)
    for k in range(n_tp - 1):
        q_copy(k).wait_recv()
    for k in range(n_tp - 1):
        pltpu.make_async_remote_copy(
            src_ref=ys.at[tp], dst_ref=ys.at[(tp + n_tp - 1 - k) % n_tp],
            send_sem=ysend.at[k], recv_sem=yrecv.at[k],
            device_id=(sp, peers[k]), device_id_type=MESH,
        ).wait_recv()
    squares = sq[0]
    for k in range(1, n_tp):
        squares = squares + sq[k]
    squares = jnp.concatenate([squares] * (LANES // 8), axis=0)
    factor = lax.rsqrt(jnp.transpose(squares)[:, :1] / (width * n_tp) + epsilon)
    loads[1].wait()
    units = hidden.shape[1]
    tile = math.gcd(units, 512)

    def up_step(c, carry):
        columns = pl.ds(pl.multiple_of(c * tile, tile), tile)
        total = jnp.dot(ys[0], up[:width, columns], preferred_element_type=F32)
        for t in range(1, n_tp):
            total = total + jnp.dot(
                ys[t], up[t * width:(t + 1) * width, columns], preferred_element_type=F32)
        total = jnp.maximum(total, 0.0) * factor
        hidden[:, columns] = (total * total).astype(BF16)

        @pl.when(c < CHUNKS)
        def _():
            event(early, c)

        return carry

    lax.fori_loop(0, units // tile, up_step, 0)

    def owners(i):
        return at(-i), at(i)

    def f_copy(i, half, owner):
        return pltpu.make_async_remote_copy(
            src_ref=pieces.at[i, half],
            dst_ref=fin.at[tp, owner % per, half],
            send_sem=fsend.at[i, half], recv_sem=frecv.at[tp, owner % per, half],
            device_id=(sp, owner // per), device_id_type=MESH,
        )

    def down_block(i, left, right):
        if narrow:
            block = jnp.concatenate([left, right], axis=0)
            half_width = left.shape[0]
            term = lax.dot_general(hidden[...], block, NT, preferred_element_type=F32)
        else:
            block = jnp.concatenate([left, right], axis=1)
            half_width = left.shape[1]
            term = jnp.dot(hidden[...], block, preferred_element_type=F32)
        term = term.astype(BF16)
        pieces[i, 0] = term[:, :half_width]
        pieces[i, 1] = term[:, half_width:]
        for half, owner in enumerate(owners(i)):

            @pl.when(owner // per != tp)
            def _():
                f_copy(i, half, owner).start()

            @pl.when(owner // per == tp)
            def _():
                fin[tp, owner % per, half] = pieces[i, half]

    for load in loads[2:]:
        load.wait()
    down_block(0, down[0, 0], down[0, 1])

    def down_step(i, carry):
        @pl.when(i <= CHUNKS)
        def _():
            event(early + 1, i - 1)

        @pl.when(i > early + 1)
        def _():
            for c in range(CHUNKS):
                landed(i - 1, c)

                @pl.when(i < n - 1)
                def _():
                    for half in range(2):
                        d_copy(i, half, c, False).start()

        down_block(i, down[i, 0], down[i, 1])
        return carry

    lax.fori_loop(1, n, down_step, 0)

    for k in range(n_tp - 1):
        source = (tp + n_tp - 1 - k) % n_tp
        for o in range(per):
            for half in range(2):
                pltpu.make_async_remote_copy(
                    src_ref=pieces.at[0, half], dst_ref=fin.at[source, o, half],
                    send_sem=fsend.at[0, half], recv_sem=frecv.at[source, o, half],
                    device_id=(sp, peers[k]), device_id_type=MESH,
                ).wait_recv()
    piece = fin.shape[4]
    for o in range(per):
        for half in range(2):
            start = (2 * o + half) * piece
            total = own_stream[:, start:start + piece]
            mixed = fin[0, o, half].astype(F32)
            for t in range(1, n_tp):
                mixed = mixed + fin[t, o, half].astype(F32)
            out_ref[:, start:start + piece] = (total + mixed).astype(BF16)

    def drain(i, carry):
        for c in range(CHUNKS):
            for half in range(2):
                d_copy(i, half, c, True).wait_send()
        return carry

    lax.fori_loop(0, n - 1, drain, 0)

    def drain_pieces(i, carry):
        for half, owner in enumerate(owners(i)):

            @pl.when(owner // per != tp)
            def _():
                f_copy(i, half, owner).wait_send()

        return carry

    lax.fori_loop(0, n, drain_pieces, 0)
    for k in range(n_tp - 1):
        p_copy(k).wait_send()
        q_copy(k).wait_send()
        y_copy(k).wait_send()


def vmem():
    return pl.BlockSpec(memory_space=pltpu.VMEM)


def hbm():
    return pl.BlockSpec(memory_space=pl.ANY)


def fused_kernel(
    n, n_tp, heads, scale, q_ref, x_ref, wk_in, wv_in, wo_ref, gain_ref, res_hbm, wu, wd,
    out_ref,
    wk_ref, wv_ref, xs, keys_ref, vals_ref, peak, acc, res_ref,
    far32, stream_ref, sbuf, sin, xbuf, xgot, mine, sq_mine, sqs, ys, up, down, hidden,
    hold, pieces, xin, finh, finz,
    zx_send, yx_send, x_recv, share_send, share_recv,
    wz_send, wy_send, wb_send, w_recv, b_recv, own_sem,
    s_send, s_recv, r_send, r_recv, y_send, y_recv, q_send, q_recv, f_send, f_recv,
    c_send, c_recv, e_send, e_recv, res_sem,
):
    sp = lax.axis_index("sp")
    tp = lax.axis_index("tp")
    nz = n // 2
    z, y = sp // 2, sp % 2
    x_at, core = tp // 2, tp % 2
    sib = tp + 1 - 2 * core
    far = (tp + 2) % n_tp
    across = sp + 1 - 2 * y
    mate = 2 * (z + 1 - 2 * (z % 2)) + y
    turn = 1 - 2 * (z // (nz // 2))
    peers = [(tp + k) % n_tp for k in range(1, n_tp)]

    def half_of(zz):
        return ((zz + 1) // 2) % 2

    def z_at(k):
        return (z + turn * k + nz) % nz

    barrier = pltpu.get_barrier_semaphore()
    greet = [(2 * ((z + k) % nz) + y, tp) for k in range(1, nz)]
    greet += [(across, tp)] + [(sp, p) for p in peers] + [(mate, p) for p in peers]
    for target in greet:
        pl.semaphore_signal(barrier, inc=1, device_id=target, device_id_type=MESH)
    pl.semaphore_wait(barrier, len(greet))

    def remote(src, dst, send, recv, target):
        return pltpu.make_async_remote_copy(
            src_ref=src, dst_ref=dst, send_sem=send, recv_sem=recv,
            device_id=target, device_id_type=MESH)

    latent = wk_ref.shape[1]
    value_width = wv_ref.shape[0] // heads
    rows = q_ref.shape[0]
    half = rows // 2
    width = stream_ref.shape[1]
    depth = wu.shape[0]
    units = up.shape[2]
    cut_u, cut_d = depth // CUTS, units // CUTS
    share_w = wd.shape[1]

    def span(r):
        return pl.ds(r * half, half)

    def zx_copy(k):
        return remote(x_ref.at[tp], xs.at[sp, tp], zx_send.at[k - 1], x_recv.at[sp],
                      (2 * z_at(k) + y, tp))

    def yx_copy(s, first):
        return remote(x_ref.at[tp] if first else xs.at[s, tp], xs.at[s, tp],
                      yx_send.at[s], x_recv.at[s], (across, tp))

    def x_landed(s):
        remote(x_ref.at[tp], xs.at[s, tp], yx_send.at[s], x_recv.at[s], (across, tp)).wait_recv()

    def share(s, k):
        return remote(xs.at[s, tp], xs.at[s, tp], share_send.at[s, k], share_recv.at[s, tp],
                      (sp, peers[k]))

    def share_all(s):
        for k in range(n_tp - 1):
            share(s, k).start()

    def share_wait(s):
        for k in range(n_tp - 1):
            remote(xs.at[s, tp], xs.at[s, peers[k]], share_send.at[s, k],
                   share_recv.at[s, peers[k]], (sp, peers[k])).wait_recv()

    def w_src(m, c, h):
        if m == 0:
            return wu.at[pl.ds(c * cut_u, cut_u), pl.ds(pl.multiple_of(h * units, LANES), units)]
        return wd.at[pl.ds(h * units + c * cut_d, cut_d)]

    def w_slot(m, side, s, c):
        if m == 0:
            return up.at[side, pl.ds(s * depth + c * cut_u, cut_u)]
        return down.at[s, pl.ds(side * units + c * cut_d, cut_d)]

    def wz_copy(m, k, c):
        there = z_at(k)
        return remote(w_src(m, c, half_of(there)), w_slot(m, core, sp, c),
                      wz_send.at[m, k - 1, c], w_recv.at[m, sp, c], (2 * there + y, tp))

    def wy_copy(m, s, c, first):
        slot = w_slot(m, core, s, c)
        return remote(w_src(m, c, half_of(z)) if first else slot, slot,
                      wy_send.at[m, s, c], w_recv.at[m, s, c], (across, tp))

    def wb_copy(m, s, c, first):
        slot = w_slot(m, core, s, c)
        return remote(w_src(m, c, half_of(z)) if first else slot, slot,
                      wb_send.at[m, s, c], b_recv.at[m, s, c], (sp, sib))

    def w_landed(m, s, c):
        slot = w_slot(m, core, s, c)
        remote(slot, slot, wy_send.at[m, s, c], w_recv.at[m, s, c], (across, tp)).wait_recv()

    def b_landed(m, s):
        for c in range(CUTS):
            slot = w_slot(m, 1 - core, s, c)
            remote(slot, slot, wb_send.at[m, s, c], b_recv.at[m, s, c], (sp, sib)).wait_recv()

    def own_copy(m):
        h = half_of(z)
        if m == 0:
            src = wu.at[:, pl.ds(pl.multiple_of(h * units, LANES), units)]
            dst = up.at[core, pl.ds(sp * depth, depth)]
        else:
            src = wd.at[pl.ds(h * units, units)]
            dst = down.at[sp, pl.ds(core * units, units)]
        return pltpu.make_async_copy(src, dst, own_sem.at[m])

    def z_send(m, k):
        for c in range(CUTS):
            wz_copy(m, k, c).start()

    def step_of(i):
        return jnp.where(i == 0, 1, nz - i) if not isinstance(i, int) else (1 if i == 0 else nz - i)

    def from_z(m, i):
        s = 2 * z_at(step_of(i)) + y
        for c in range(CUTS):
            w_landed(m, s, c)
            wy_copy(m, s, c, False).start()
            wb_copy(m, s, c, False).start()

    def from_y(m, s):
        for c in range(CUTS):
            w_landed(m, s, c)
            wb_copy(m, s, c, False).start()

    def y_origin(i):
        return 2 * z_at(step_of(i)) + 1 - y

    for k in range(1, nz):
        zx_copy(k).start()
    yx_copy(sp, True).start()
    for k in [nz - 1] + list(range(1, nz - 1)):
        z_send(0, k)
    for m in range(2):
        own_copy(m).start()
    for m in range(2):
        for c in range(CUTS):
            wb_copy(m, sp, c, True).start()
    res_copy = pltpu.make_async_copy(
        res_hbm.at[:, pl.ds(pl.multiple_of(tp * width, LANES), width)], res_ref, res_sem)
    res_copy.start()
    wk_ref[...] = jnp.transpose(wk_in[...].astype(F32)).astype(BF16)
    wv_ref[...] = jnp.transpose(wv_in[...].astype(F32)).astype(BF16)
    peak[...] = jnp.full(peak.shape, -1e30, F32)
    acc[...] = jnp.zeros(acc.shape, F32)
    for t in range(n_tp):
        xs[sp, t] = x_ref[t]

    def project_keys(s):
        block = jnp.concatenate([xs[s, t] for t in range(n_tp)], axis=1)
        lat = block[:latent]
        rot = block[latent:]
        count = block.shape[1]
        k_all = jnp.dot(wk_ref[...], lat, preferred_element_type=F32).astype(BF16)
        v_all = jnp.dot(wv_ref[...], lat, preferred_element_type=F32).astype(BF16)
        k_pad = jnp.zeros((LANES - UNROTATED_WIDTH - rot.shape[0], count), BF16)
        ones = jnp.ones((16, count), BF16)
        v_pad = jnp.zeros((LANES - value_width - 16, count), BF16)
        for h in range(heads):
            keys_ref[s, h] = jnp.concatenate(
                [k_all[h * UNROTATED_WIDTH:(h + 1) * UNROTATED_WIDTH], rot, k_pad], axis=0)
            vals_ref[s, h] = jnp.concatenate(
                [v_all[h * value_width:(h + 1) * value_width], ones, v_pad], axis=0)

    def attend(s, r, size):
        lines = pl.ds(r * half, size)
        for h in range(heads):
            score = jnp.dot(q_ref[lines, h * LANES:(h + 1) * LANES], keys_ref[s, h],
                            preferred_element_type=F32)
            old = peak[h, lines]
            new = jnp.maximum(old, jnp.max(score, axis=1, keepdims=True))
            p = jnp.exp2((score - new) * scale).astype(BF16)
            acc[h, lines] = acc[h, lines] * jnp.exp2((old - new) * scale) + lax.dot_general(
                p, vals_ref[s, h], NT, preferred_element_type=F32)
            peak[h, lines] = new

    def block_at(b):
        flip = (b - 2) // (nz - 1)
        off = (b - 2) % (nz - 1) + 1
        there = 2 * ((z + off) % nz) + (y + flip) % 2
        return there

    def s_copy(r):
        return remote(sbuf.at[r], sin.at[r], s_send.at[r], s_recv.at[r], (sp, sib))

    def r_copy(r):
        return remote(xbuf.at[r], xgot.at[r], r_send.at[r], r_recv.at[r], (sp, far))

    def project(r):
        group = []
        for h in range(heads):
            a = acc[h, span(r)]
            group.append((a[:, :value_width] / a[:, value_width:value_width + 1]).astype(BF16))
        attended = jnp.concatenate(group, axis=1)

        def quarter(t):
            return jnp.dot(attended, wo_ref[:, pl.ds(pl.multiple_of(t * width, LANES), width)],
                           preferred_element_type=F32)

        sbuf[r, 0] = quarter(sib).astype(BF16)
        sbuf[r, 1] = quarter((sib + 2) % n_tp).astype(BF16)
        s_copy(r).start()
        far32[span(r)] = quarter(far)
        stream_ref[span(r)] = quarter(tp)

    def relay(r):
        s_copy(r).wait_recv()
        xbuf[r] = (far32[span(r)] + sin[r, 1].astype(F32)).astype(BF16)
        r_copy(r).start()

    home_far = 2 * (1 - x_at)

    def columns(t):
        return pl.ds(pl.multiple_of(t * width, LANES), width)

    def y_copy(r, which):
        target = ((sp, sib), (sp, home_far), (mate, 2 * x_at + 1))[which]
        return remote(mine.at[span(r)], ys.at[span(r), columns(tp)],
                      y_send.at[r, which], y_recv.at[r, tp], target)

    def q_copy(r, which):
        target = ((sp, sib), (sp, home_far), (mate, 2 * x_at + 1), (mate, home_far + 1))[which]
        return remote(sq_mine.at[r], sqs.at[r, tp], q_send.at[r, which], q_recv.at[r, tp], target)

    def f_copy(r, i):
        t = 2 * x_at + i
        return remote(ys.at[span(r), columns(t)], ys.at[span(r), columns(t)],
                      f_send.at[r, i], y_recv.at[r, t], (sp, home_far + 1))

    def y_wait(r, t):
        remote(mine.at[span(r)], ys.at[span(r), columns(t)],
               y_send.at[r, 1], y_recv.at[r, t], (sp, home_far)).wait_recv()

    def q_wait(r, t):
        remote(sq_mine.at[r], sqs.at[r, t], q_send.at[r, 1], q_recv.at[r, t],
               (sp, home_far)).wait_recv()

    def settle(r):
        r_copy(r).wait_recv()
        stream = stream_ref[span(r)] + sin[r, 0].astype(F32) + xgot[r].astype(F32)
        stream = stream + res_ref[span(r)].astype(F32)
        stream_ref[span(r)] = stream
        shard = (stream * gain_ref[tp]).astype(BF16)
        mine[span(r)] = shard
        total = jnp.sum(stream * stream, axis=1, keepdims=True)
        squares = jnp.transpose(jnp.broadcast_to(total, (half, LANES)))[:8]
        sq_mine[r] = squares

        @pl.when(core == 0)
        def _():
            ys[span(r), columns(tp)] = shard
            sqs[r, tp] = squares

        q_copy(r, 2).start()
        y_copy(r, 2).start()
        q_copy(r, 3).start()
        q_copy(r, 1).start()
        y_copy(r, 1).start()

        @pl.when(core == 1)
        def _():
            q_copy(r, 0).start()
            y_copy(r, 0).start()

    def pass_on(r):
        @pl.when(core == 1)
        def _():
            for i in range(2):
                y_wait(r, 2 * x_at + i)
                f_copy(r, i).start()

    def gathered(r):
        @pl.when(core == 1)
        def _():
            for i in range(2):
                y_wait(r, home_far + i)
            for t in range(n_tp):
                q_wait(r, t)

        @pl.when(core == 0)
        def _():
            for t in peers:
                y_wait(r, t)
                q_wait(r, t)

    project_keys(sp)
    attend(sp, 0, half)
    x_landed(across)
    share_all(across)
    attend(sp, 1, half)
    for off in range(1, nz):
        s = 2 * ((z + off) % nz) + y
        x_landed(s)
        yx_copy(s, False).start()
        share_all(s)
    for m in range(2):
        for c in range(CUTS):
            wy_copy(m, sp, c, True).start()

    split = n // 2

    def first_blocks(b, carry):
        s = jnp.where(b == 1, across, block_at(b))
        share_wait(s)
        project_keys(s)
        attend(s, 0, rows)

        @pl.when(b == 1)
        def _():
            for off in range(1, nz):
                there = 2 * ((z + off) % nz) + 1 - y
                x_landed(there)
                share_all(there)

        return carry

    def second_blocks(b, carry):
        s = block_at(b)
        share_wait(s)
        project_keys(s)
        attend(s, 0, half)

        @pl.when(b == split + 1)
        def _():
            from_z(0, 0)

        @pl.when(b == n - 1)
        def _():
            from_z(0, 1)

        return carry

    def third_blocks(b, carry):
        attend(block_at(b), 1, half)

        @pl.when(b == split)
        def _():
            relay(0)
            from_y(0, across)

        @pl.when(b == split + 2)
        def _():
            settle(0)
            z_send(1, 1)

        @pl.when(b == n - 1)
        def _():
            from_y(0, y_origin(0))

        return carry

    lax.fori_loop(1, split, first_blocks, 0)
    lax.fori_loop(split, n, second_blocks, 0)
    res_copy.wait()
    project(0)
    lax.fori_loop(split, n, third_blocks, 0)
    project(1)
    relay(1)
    pass_on(0)
    settle(1)
    for k in [nz - 1] + list(range(2, nz - 1)):
        z_send(1, k)
    for i in range(2, nz - 1):
        from_z(0, i)
    pass_on(1)
    for i in range(1, nz - 1):
        from_y(0, y_origin(i))
    from_z(1, 0)
    own_copy(0).wait()
    for s in range(n):
        b_landed(0, s)
    gathered(0)
    gathered(1)

    factors = []
    for r in range(2):
        squares = sqs[r, 0]
        for t in range(1, n_tp):
            squares = squares + sqs[r, t]
        squares = jnp.concatenate([squares] * (LANES // 8), axis=0)
        factors.append(jnp.transpose(squares)[:, :1])
    factor = lax.rsqrt(jnp.concatenate(factors, axis=0) / (width * n_tp) + epsilon)
    tile = math.gcd(units, 512)
    tiles = units // tile

    def up_step(i, carry):
        within = pl.ds(pl.multiple_of((i % tiles) * tile, tile), tile)
        total = jnp.dot(ys[...], up[i // tiles, :, within], preferred_element_type=F32)
        total = jnp.maximum(total, 0.0) * factor
        hidden[:, pl.ds(pl.multiple_of(i * tile, tile), tile)] = (total * total).astype(BF16)
        return carry

    lax.fori_loop(0, 2 * tiles, up_step, 0)

    per = n // n_tp

    def order(j):
        i = (j - 2) // 2
        there = 2 * z_at(step_of(i)) + (y + j) % 2
        return jnp.where(j == 0, sp, jnp.where(j == 1, across, there))

    def c_copy(s):
        return remote(pieces.at[s], xin.at[s % nz], c_send.at[s], c_recv.at[s % nz], (sp, far))

    def e_copy(s):
        return remote(pieces.at[s], finh.at[s % per], e_send.at[s], e_recv.at[0, s % per],
                      (sp, s // per))

    def g_copy(s):
        return remote(pieces.at[s], finz.at[s % per], e_send.at[s], e_recv.at[1, s % per],
                      (mate, s // per))

    def owner_is_here(s):
        return s // nz == x_at

    def finish(s):
        @pl.when(owner_is_here(s))
        def _():
            c_copy(s).wait_recv()
            value = (hold[s % nz] + xin[s % nz].astype(F32)).astype(BF16)

            @pl.when(core == 1)
            def _():
                pieces[s] = value
                g_copy(s).start()

            @pl.when(core == 0)
            def _():
                @pl.when(s // per == tp)
                def _():
                    finh[s % per] = value

                @pl.when(s // per != tp)
                def _():
                    pieces[s] = value
                    e_copy(s).start()

    own_copy(1).wait()

    def down_step(j, carry):
        s = order(j)
        i = (j - 2) // 2

        @pl.when(j % 2 == 1)
        def _():
            from_y(1, s)

        @pl.when((j % 2 == 0) & (j >= 4))
        def _():
            from_z(1, i)

        b_landed(1, s)
        term = jnp.dot(hidden[...], down[s], preferred_element_type=F32)

        @pl.when(owner_is_here(s))
        def _():
            hold[s % nz] = term

        @pl.when(s // nz != x_at)
        def _():
            pieces[s] = term.astype(BF16)
            c_copy(s).start()

        @pl.when(j > 0)
        def _():
            finish(order(j - 1))

        return carry

    lax.fori_loop(0, n, down_step, 0)
    finish(order(n - 1))

    for o in range(per):
        s = tp * per + o
        g_copy(s).wait_recv()

        @pl.when(core == 1)
        def _():
            e_copy(s).wait_recv()

        cols = slice(o * share_w, (o + 1) * share_w)
        out_ref[:, cols] = (
            stream_ref[:, cols] + (finh[o].astype(F32) + finz[o].astype(F32))).astype(BF16)

    for k in range(1, nz):
        zx_copy(k).wait_send()
        for m in range(2):
            for c in range(CUTS):
                wz_copy(m, k, c).wait_send()
    yx_copy(sp, True).wait_send()
    for k in range(n_tp - 1):
        share(across, k).wait_send()
    for off in range(1, nz):
        s = 2 * ((z + off) % nz) + y
        yx_copy(s, False).wait_send()
        for k in range(n_tp - 1):
            share(s, k).wait_send()
            share(2 * ((z + off) % nz) + 1 - y, k).wait_send()
    for off in range(nz):
        s = 2 * ((z + off) % nz) + y
        for m in range(2):
            for c in range(CUTS):
                wy_copy(m, s, c, False).wait_send()

    def drain(s, carry):
        for m in range(2):
            for c in range(CUTS):
                wb_copy(m, s, c, False).wait_send()

        @pl.when(s // nz != x_at)
        def _():
            c_copy(s).wait_send()

        @pl.when(owner_is_here(s) & ((core == 1) | (s // per != tp)))
        def _():
            g_copy(s).wait_send()

        return carry

    lax.fori_loop(0, n, drain, 0)
    for r in range(2):
        s_copy(r).wait_send()
        r_copy(r).wait_send()
        for which in range(1, 3):
            y_copy(r, which).wait_send()
        for which in range(1, 4):
            q_copy(r, which).wait_send()

        @pl.when(core == 1)
        def _():
            y_copy(r, 0).wait_send()
            q_copy(r, 0).wait_send()
            for i in range(2):
                f_copy(r, i).wait_send()


def fused(n, n_tp, heads, scale, queries, x, key_up, value_up, w_out, gain, residual, w_up, w_down):
    rows, model = residual.shape
    depth, units = w_up.shape[0], w_up.shape[1] // 2
    share_w = w_down.shape[1]
    width = model // n_tp
    wide = x.shape[1]
    half, nz, per = rows // 2, n // 2, n // n_tp
    dma = pltpu.SemaphoreType.DMA
    return pl.pallas_call(
        functools.partial(fused_kernel, n, n_tp, heads, scale),
        out_shape=jax.ShapeDtypeStruct((rows, width), BF16),
        in_specs=[vmem()] * 6 + [hbm()] * 3,
        out_specs=vmem(),
        scratch_shapes=[
            pltpu.VMEM(key_up.shape[::-1], BF16),
            pltpu.VMEM(value_up.shape[::-1], BF16),
            pltpu.VMEM((n, n_tp, wide, rows // n_tp), BF16),
            pltpu.VMEM((n, heads, LANES, rows), BF16),
            pltpu.VMEM((n, heads, LANES, rows), BF16),
            pltpu.VMEM((heads, rows, 1), F32),
            pltpu.VMEM((heads, rows, LANES), F32),
            pltpu.VMEM((rows, width), BF16),
            pltpu.VMEM((rows, width), F32),
            pltpu.VMEM((rows, width), F32),
            pltpu.VMEM((2, 2, half, width), BF16),
            pltpu.VMEM((2, 2, half, width), BF16),
            pltpu.VMEM((2, half, width), BF16),
            pltpu.VMEM((2, half, width), BF16),
            pltpu.VMEM((rows, width), BF16),
            pltpu.VMEM((2, 8, half), F32),
            pltpu.VMEM((2, n_tp, 8, half), F32),
            pltpu.VMEM((rows, model), BF16),
            pltpu.VMEM((2, model, units), BF16),
            pltpu.VMEM((n, 2 * units, share_w), BF16),
            pltpu.VMEM((rows, 2 * units), BF16),
            pltpu.VMEM((nz, rows, share_w), F32),
            pltpu.VMEM((n, rows, share_w), BF16),
            pltpu.VMEM((nz, rows, share_w), BF16),
            pltpu.VMEM((per, rows, share_w), BF16),
            pltpu.VMEM((per, rows, share_w), BF16),
            dma((nz - 1,)), dma((n,)), dma((n,)), dma((n, n_tp - 1)), dma((n, n_tp)),
            dma((2, nz - 1, CUTS)), dma((2, n, CUTS)), dma((2, n, CUTS)),
            dma((2, n, CUTS)), dma((2, n, CUTS)), dma((2,)),
            dma((2,)), dma((2,)), dma((2,)), dma((2,)),
            dma((2, 3)), dma((2, n_tp)), dma((2, 4)), dma((2, n_tp)),
            dma((2, 2)), dma((2, 2)),
            dma((n,)), dma((nz,)), dma((n,)), dma((2, per)), dma,
        ],
        compiler_params=pltpu.CompilerParams(
            collective_id=2, has_side_effects=True, vmem_limit_bytes=62 * 2**20),
        name="layer",
    )(queries, x, key_up, value_up, w_out, gain, residual, w_up, w_down)


def on_device(
    n,
    n_tp,
    residual_in,
    queries_nope,
    queries_rope,
    latents,
    rope_keys,
    latent_norm_gain,
    key_up_weight,
    value_up_weight,
    w_out,
    norm_gain,
    w_up,
    w_down,
):
    rows, model = residual_in.shape
    heads = key_up_weight.shape[1] // UNROTATED_WIDTH
    value_width = value_up_weight.shape[1] // heads
    positions = lax.axis_index("sp") * rows + jnp.arange(rows, dtype=jnp.int32)
    phases = rope_phases(positions, ROPE)
    q_rot = rotate(
        queries_rope.astype(F32).reshape(rows, heads, ROPE), phases[:, None, :]
    ).astype(BF16)
    queries = jnp.concatenate(
        [
            queries_nope.reshape(rows, heads, UNROTATED_WIDTH),
            q_rot,
            jnp.zeros((rows, heads, LANES - UNROTATED_WIDTH - ROPE), BF16),
        ],
        axis=2,
    ).reshape(rows, heads * LANES)
    lat_norm = rms_scale(latents.astype(F32), latent_norm_gain).astype(BF16)
    key_rot = rotate(rope_keys.astype(F32), phases).astype(BF16)
    x = jnp.concatenate([lat_norm, key_rot], axis=1)
    wide = x.shape[1]
    x = jnp.transpose(x.reshape(n_tp, rows // n_tp, wide), (0, 2, 1))

    width = model // n_tp
    depth, units = w_up.shape
    scale = math.log2(math.e) / math.sqrt(UNROTATED_WIDTH + ROPE)
    lined = depth % (16 * CUTS) == 0 and w_down.shape[1] % LANES == 0 and rows % 256 == 0
    if n % 4 == 0 and n > 4 and n_tp == 4 and n % (2 * n_tp) == 0 and lined:
        return fused(
            n, n_tp, heads, scale, queries, x, key_up_weight, value_up_weight, w_out,
            norm_gain.reshape(n_tp, 1, width), residual_in, w_up, w_down)
    dma = pltpu.SemaphoreType.DMA
    part, full = pl.pallas_call(
        functools.partial(
            attention_kernel, n, n_tp, heads,
            math.log2(math.e) / math.sqrt(UNROTATED_WIDTH + ROPE)),
        out_shape=(
            jax.ShapeDtypeStruct((n_tp, rows, width), BF16),
            jax.ShapeDtypeStruct((n, 2, CHUNKS, depth // 2 // CHUNKS, units), BF16),
        ),
        in_specs=[vmem()] * 5 + [hbm()],
        out_specs=(vmem(), hbm()),
        scratch_shapes=[
            pltpu.VMEM(key_up_weight.shape[::-1], BF16),
            pltpu.VMEM(value_up_weight.shape[::-1], BF16),
            pltpu.VMEM((n, n_tp, wide, rows // n_tp), BF16),
            pltpu.VMEM((heads, rows, 1), F32),
            pltpu.VMEM((heads, rows, LANES), F32),
            dma((n - 1,)), dma((n - 1,)),
            dma((n, n_tp - 1)), dma((n, n_tp - 1)),
            dma((n - 1, 2, CHUNKS)), dma((n - 1, 2, CHUNKS)), dma,
        ],
        compiler_params=pltpu.CompilerParams(
            collective_id=0, has_side_effects=True, vmem_limit_bytes=56 * 2**20),
        name="attend",
    )(
        queries, x, key_up_weight, value_up_weight,
        w_out, w_up.reshape(2, CHUNKS, depth // 2 // CHUNKS, units),
    )

    hidden_units, share = w_down.shape
    narrow = (share // 2) % LANES != 0
    if narrow:
        down_in = jnp.transpose(w_down.reshape(hidden_units, 2, share // 2), (1, 2, 0))
        half_shape = (share // 2, hidden_units)
    else:
        down_in = w_down
        half_shape = (hidden_units, share // 2)
    per = n // n_tp
    return pl.pallas_call(
        functools.partial(feed_kernel, n, n_tp, narrow),
        out_shape=jax.ShapeDtypeStruct((rows, width), BF16),
        in_specs=[vmem(), hbm(), vmem(), hbm(), hbm()],
        out_specs=vmem(),
        scratch_shapes=[
            pltpu.VMEM((rows, width), BF16),
            pltpu.VMEM((model, units), BF16),
            pltpu.VMEM((n, 2) + half_shape, BF16),
            pltpu.VMEM((n_tp - 1, rows, width), BF16),
            pltpu.VMEM((n_tp, rows, width), BF16),
            pltpu.VMEM((n_tp, 8, rows), F32),
            pltpu.VMEM((rows, width), F32),
            pltpu.VMEM((rows, units), BF16),
            pltpu.VMEM((n, 2, rows, share // 2), BF16),
            pltpu.VMEM((n_tp, per, 2, rows, share // 2), BF16),
            dma((n - 1, 2, CHUNKS)), dma((n - 1, 2, CHUNKS)),
            dma((n_tp - 1,)), dma((n_tp - 1,)),
            dma((n_tp - 1,)), dma((n_tp - 1,)),
            dma((n_tp - 1,)), dma((n_tp - 1,)),
            dma((n, 2)), dma((n_tp, per, 2)),
            dma((4,)),
        ],
        compiler_params=pltpu.CompilerParams(
            collective_id=1, has_side_effects=True, vmem_limit_bytes=60 * 2**20),
        name="feed",
    )(part, residual_in, norm_gain.reshape(n_tp, 1, width), full.reshape(model, units), down_in)


def solution(mesh):
    in_specs = (
        P("sp", None),
        P("sp", "tp"),
        P("sp", "tp"),
        P("sp", None),
        P("sp", None),
        P(),
        P(None, "tp"),
        P(None, "tp"),
        P("tp", None),
        P(),
        P("sp", "tp"),
        P("tp", "sp"),
    )
    out_specs = P("sp", "tp")
    return jax.shard_map(
        functools.partial(on_device, mesh.shape["sp"], mesh.shape["tp"]),
        mesh=mesh, in_specs=in_specs, out_specs=out_specs, check_vma=False,
    )
```

```python
import functools
import math

import jax
import jax.numpy as jnp
import numpy as np
from jax import lax
from jax.experimental import pallas as pl
from jax.experimental.pallas import tpu as pltpu
from jax.sharding import PartitionSpec as P

UNROTATED_WIDTH = 64
ROPE = 32
LANES = 128
CHUNKS = 4
CUTS = 2
LAG = 3

rope_base = 10000.0
epsilon = 1e-06
F32 = jnp.float32
BF16 = jnp.bfloat16
MESH = pl.DeviceIdType.MESH
NT = (((1,), (1,)), ((), ()))


def rotate(vectors, phases):
    half_width = vectors.shape[-1] // 2
    first_half = vectors[..., :half_width]
    second_half = vectors[..., half_width:]
    cosine = jnp.cos(phases)
    sine = jnp.sin(phases)
    return jnp.concatenate(
        [first_half * cosine - second_half * sine, second_half * cosine + first_half * sine],
        axis=-1,
    )


def rope_phases(positions, width):
    inverse = 1.0 / rope_base ** (jnp.arange(0, width, 2, dtype=jnp.float32) / width)
    return positions.astype(jnp.float32)[:, None] * inverse[None, :]


def rms_scale(vectors, gain_vec):
    return (
        vectors
        * lax.rsqrt(jnp.mean(vectors * vectors, axis=-1, keepdims=True) + epsilon)
        * gain_vec
    )


def ring_of(index, n):
    return index // 2 + (index % 2) * (n - 1 - 2 * (index // 2))


def index_of(place, n):
    return 2 * place + (place // (n // 2)) * (2 * n - 1 - 4 * place)


def ring_ids(n):
    place = ring_of(lax.axis_index("sp"), n)

    def at(offset):
        return index_of((place + offset + 2 * n) % n, n)

    return at


def attention_kernel(
    n, n_tp, heads, scale, q_ref, x_ref, wk_in, wv_in, wo_ref, wu_ref,
    part_ref, full_ref,
    wk_ref, wv_ref, xs, peak, acc, xsend, xrecv, ssend, srecv, wsend, wrecv, own_sem,
):
    at = ring_ids(n)
    tp = lax.axis_index("tp")
    me = lax.axis_index("sp")
    to = ((at(1), tp), (at(-1), tp))
    peers = [(tp + k) % n_tp for k in range(1, n_tp)]
    onward = (at(1 - 2 * (tp % 2)), tp)
    barrier = pltpu.get_barrier_semaphore()
    for target in list(to) + [(me, p) for p in peers]:
        pl.semaphore_signal(barrier, inc=1, device_id=target, device_id_type=MESH)
    pl.semaphore_wait(barrier, 2 + n_tp - 1)

    latent = wk_ref.shape[1]
    value_width = wv_ref.shape[0] // heads

    def x_copy(step, src):
        return pltpu.make_async_remote_copy(
            src_ref=src, dst_ref=xs.at[step + 1, tp],
            send_sem=xsend.at[step], recv_sem=xrecv.at[step],
            device_id=onward, device_id_type=MESH,
        )

    def share(step, k):
        return pltpu.make_async_remote_copy(
            src_ref=xs.at[step, tp], dst_ref=xs.at[step, tp],
            send_sem=ssend.at[step, k], recv_sem=srecv.at[step, k],
            device_id=(me, peers[k]), device_id_type=MESH,
        )

    def share_wait(step):
        for k in range(n_tp - 1):
            pltpu.make_async_remote_copy(
                src_ref=xs.at[step, tp], dst_ref=xs.at[step, (tp + n_tp - 1 - k) % n_tp],
                send_sem=ssend.at[step, k], recv_sem=srecv.at[step, k],
                device_id=(me, peers[k]), device_id_type=MESH,
            ).wait_recv()

    def w_copy(step, half, c, first):
        owner = at(-step) if half == 0 else at(step)
        return pltpu.make_async_remote_copy(
            src_ref=wu_ref.at[half, c] if first else full_ref.at[owner, half, c],
            dst_ref=full_ref.at[owner, half, c],
            send_sem=wsend.at[step, half, c], recv_sem=wrecv.at[step, half, c],
            device_id=to[half], device_id_type=MESH,
        )

    x_copy(0, x_ref.at[tp]).start()
    for c in range(CHUNKS):
        for half in range(2):
            w_copy(0, half, c, True).start()
    own = pltpu.make_async_copy(wu_ref, full_ref.at[me], own_sem)
    own.start()
    wk_ref[...] = jnp.transpose(wk_in[...].astype(F32)).astype(BF16)
    wv_ref[...] = jnp.transpose(wv_in[...].astype(F32)).astype(BF16)
    peak[...] = jnp.full(peak.shape, -1e30, F32)
    acc[...] = jnp.zeros(acc.shape, F32)

    def attend(blocks):
        block = jnp.concatenate(blocks, axis=1)
        lat = block[:latent]
        rot = block[latent:]
        keys = block.shape[1]
        k_all = jnp.dot(wk_ref[...], lat, preferred_element_type=F32).astype(BF16)
        v_all = jnp.dot(wv_ref[...], lat, preferred_element_type=F32).astype(BF16)
        k_pad = jnp.zeros((LANES - UNROTATED_WIDTH - rot.shape[0], keys), BF16)
        ones = jnp.ones((16, keys), BF16)
        v_pad = jnp.zeros((LANES - value_width - 16, keys), BF16)
        for h in range(heads):
            k_h = jnp.concatenate(
                [k_all[h * UNROTATED_WIDTH:(h + 1) * UNROTATED_WIDTH], rot, k_pad], axis=0)
            v_h = jnp.concatenate(
                [v_all[h * value_width:(h + 1) * value_width], ones, v_pad], axis=0)
            s = jnp.dot(q_ref[:, h * LANES:(h + 1) * LANES], k_h, preferred_element_type=F32)
            old = peak[h]
            new = jnp.maximum(old, jnp.max(s, axis=1, keepdims=True))
            p = jnp.exp2((s - new) * scale).astype(BF16)
            acc[h] = acc[h] * jnp.exp2((old - new) * scale) + lax.dot_general(
                p, v_h, NT, preferred_element_type=F32)
            peak[h] = new

    def turn(i, carry):
        x_copy(i - 1, x_ref.at[tp]).wait_recv()
        x_copy(i, xs.at[i, tp]).start()
        for k in range(n_tp - 1):
            share(i, k).start()
        for c in range(CHUNKS):
            for half in range(2):
                w_copy(i - 1, half, c, True).wait_recv()
                w_copy(i, half, c, False).start()

        @pl.when(i > 1)
        def _():
            share_wait(i - 1)
            attend([xs[i - 1, t] for t in range(n_tp)])

        return carry

    attend([x_ref[t] for t in range(n_tp)])
    lax.fori_loop(1, n - 1, turn, 0)
    x_copy(n - 2, x_ref.at[tp]).wait_recv()
    for k in range(n_tp - 1):
        share(n - 1, k).start()

    def last(i, carry):
        share_wait(i)
        attend([xs[i, t] for t in range(n_tp)])
        return carry

    lax.fori_loop(n - 2, n, last, 0)

    width = part_ref.shape[2]
    group = []
    for h in range(heads):
        a = acc[h]
        group.append((a[:, :value_width] / a[:, value_width:value_width + 1]).astype(BF16))
    attended = jnp.concatenate(group, axis=1)
    for j in range(part_ref.shape[0]):
        part_ref[j] = jnp.dot(
            attended, wo_ref[:, j * width:(j + 1) * width], preferred_element_type=F32
        ).astype(BF16)

    own.wait()
    for c in range(CHUNKS):
        for half in range(2):
            w_copy(n - 2, half, c, True).wait_recv()

    def drain(i, carry):
        x_copy(i, x_ref.at[tp]).wait_send()
        for k in range(n_tp - 1):
            share(i + 1, k).wait_send()
        for c in range(CHUNKS):
            for half in range(2):
                w_copy(i, half, c, True).wait_send()
        return carry

    lax.fori_loop(0, n - 1, drain, 0)


def feed_kernel(
    n, n_tp, narrow, part_ref, res_hbm, gain_ref, up_hbm, wd_hbm,
    out_ref,
    res_ref, up, down, parts, ys, sq, own_stream, hidden, pieces, fin,
    dsend, drecv, psend, precv, ysend, yrecv, qsend, qrecv, fsend, frecv, local,
):
    at = ring_ids(n)
    tp = lax.axis_index("tp")
    sp = lax.axis_index("sp")
    to = ((at(1), tp), (at(-1), tp))
    peers = [(tp + k) % n_tp for k in range(1, n_tp)]
    barrier = pltpu.get_barrier_semaphore()
    for target in list(to) + [(sp, p) for p in peers]:
        pl.semaphore_signal(barrier, inc=1, device_id=target, device_id_type=MESH)
    pl.semaphore_wait(barrier, 2 + n_tp - 1)

    rows, width = res_ref.shape
    per = n // n_tp

    lines = down.shape[2] // CHUNKS

    def own_half(half):
        if narrow:
            return wd_hbm.at[half]
        return wd_hbm.at[:, half * down.shape[3]:(half + 1) * down.shape[3]]

    def d_copy(step, half, c, first):
        span = pl.ds(c * lines, lines)
        if not first:
            src = down.at[step, half, span]
        elif narrow:
            src = wd_hbm.at[half, span]
        else:
            src = wd_hbm.at[span, half * down.shape[3]:(half + 1) * down.shape[3]]
        return pltpu.make_async_remote_copy(
            src_ref=src, dst_ref=down.at[step + 1, half, span],
            send_sem=dsend.at[step, half, c], recv_sem=drecv.at[step, half, c],
            device_id=to[half], device_id_type=MESH,
        )

    def p_copy(k):
        peer = peers[k]
        return pltpu.make_async_remote_copy(
            src_ref=part_ref.at[peer], dst_ref=parts.at[k],
            send_sem=psend.at[k], recv_sem=precv.at[k],
            device_id=(sp, peer), device_id_type=MESH,
        )

    def y_copy(k):
        return pltpu.make_async_remote_copy(
            src_ref=ys.at[tp], dst_ref=ys.at[tp],
            send_sem=ysend.at[k], recv_sem=yrecv.at[k],
            device_id=(sp, peers[k]), device_id_type=MESH,
        )

    def q_copy(k):
        return pltpu.make_async_remote_copy(
            src_ref=sq.at[0], dst_ref=sq.at[k + 1],
            send_sem=qsend.at[k], recv_sem=qrecv.at[k],
            device_id=(sp, peers[k]), device_id_type=MESH,
        )

    def landed(step, c):
        for half in range(2):
            d_copy(step, half, c, True).wait_recv()

    def event(step, c):
        landed(step - 1, c)
        for half in range(2):
            d_copy(step, half, c, False).start()

    def events(first, last):
        for tick in range(first, last):
            event(1 + tick // CHUNKS, tick % CHUNKS)

    for c in range(CHUNKS):
        for half in range(2):
            d_copy(0, half, c, True).start()
    for k in range(n_tp - 1):
        p_copy(k).start()
    loads = [
        pltpu.make_async_copy(
            res_hbm.at[:, pl.ds(pl.multiple_of(tp * width, LANES), width)], res_ref, local.at[0]),
        pltpu.make_async_copy(up_hbm, up, local.at[1]),
        pltpu.make_async_copy(own_half(0), down.at[0, 0], local.at[2]),
        pltpu.make_async_copy(own_half(1), down.at[0, 1], local.at[3]),
    ]
    for load in loads:
        load.start()

    early = 4
    events(0, 6)
    for k in range(n_tp - 1):
        p_copy(k).wait_recv()
    loads[0].wait()
    stream = part_ref[tp].astype(F32)
    for k in range(n_tp - 1):
        stream = stream + parts[k].astype(F32)
    stream = stream + res_ref[...].astype(F32)
    own_stream[...] = stream
    ys[tp] = (stream * gain_ref[tp]).astype(BF16)
    total = jnp.sum(stream * stream, axis=1, keepdims=True)
    sq[0] = jnp.transpose(jnp.broadcast_to(total, (rows, LANES)))[:8]
    for k in range(n_tp - 1):
        q_copy(k).start()
        y_copy(k).start()
    events(6, 12)
    for k in range(n_tp - 1):
        q_copy(k).wait_recv()
    for k in range(n_tp - 1):
        pltpu.make_async_remote_copy(
            src_ref=ys.at[tp], dst_ref=ys.at[(tp + n_tp - 1 - k) % n_tp],
            send_sem=ysend.at[k], recv_sem=yrecv.at[k],
            device_id=(sp, peers[k]), device_id_type=MESH,
        ).wait_recv()
    squares = sq[0]
    for k in range(1, n_tp):
        squares = squares + sq[k]
    squares = jnp.concatenate([squares] * (LANES // 8), axis=0)
    factor = lax.rsqrt(jnp.transpose(squares)[:, :1] / (width * n_tp) + epsilon)
    loads[1].wait()
    units = hidden.shape[1]
    tile = math.gcd(units, 512)

    def up_step(c, carry):
        columns = pl.ds(pl.multiple_of(c * tile, tile), tile)
        total = jnp.dot(ys[0], up[:width, columns], preferred_element_type=F32)
        for t in range(1, n_tp):
            total = total + jnp.dot(
                ys[t], up[t * width:(t + 1) * width, columns], preferred_element_type=F32)
        total = jnp.maximum(total, 0.0) * factor
        hidden[:, columns] = (total * total).astype(BF16)

        @pl.when(c < CHUNKS)
        def _():
            event(early, c)

        return carry

    lax.fori_loop(0, units // tile, up_step, 0)

    def owners(i):
        return at(-i), at(i)

    def f_copy(i, half, owner):
        return pltpu.make_async_remote_copy(
            src_ref=pieces.at[i, half],
            dst_ref=fin.at[tp, owner % per, half],
            send_sem=fsend.at[i, half], recv_sem=frecv.at[tp, owner % per, half],
            device_id=(sp, owner // per), device_id_type=MESH,
        )

    def down_block(i, left, right):
        if narrow:
            block = jnp.concatenate([left, right], axis=0)
            half_width = left.shape[0]
            term = lax.dot_general(hidden[...], block, NT, preferred_element_type=F32)
        else:
            block = jnp.concatenate([left, right], axis=1)
            half_width = left.shape[1]
            term = jnp.dot(hidden[...], block, preferred_element_type=F32)
        term = term.astype(BF16)
        pieces[i, 0] = term[:, :half_width]
        pieces[i, 1] = term[:, half_width:]
        for half, owner in enumerate(owners(i)):

            @pl.when(owner // per != tp)
            def _():
                f_copy(i, half, owner).start()

            @pl.when(owner // per == tp)
            def _():
                fin[tp, owner % per, half] = pieces[i, half]

    for load in loads[2:]:
        load.wait()
    down_block(0, down[0, 0], down[0, 1])

    def down_step(i, carry):
        @pl.when(i <= CHUNKS)
        def _():
            event(early + 1, i - 1)

        @pl.when(i > early + 1)
        def _():
            for c in range(CHUNKS):
                landed(i - 1, c)

                @pl.when(i < n - 1)
                def _():
                    for half in range(2):
                        d_copy(i, half, c, False).start()

        down_block(i, down[i, 0], down[i, 1])
        return carry

    lax.fori_loop(1, n, down_step, 0)

    for k in range(n_tp - 1):
        source = (tp + n_tp - 1 - k) % n_tp
        for o in range(per):
            for half in range(2):
                pltpu.make_async_remote_copy(
                    src_ref=pieces.at[0, half], dst_ref=fin.at[source, o, half],
                    send_sem=fsend.at[0, half], recv_sem=frecv.at[source, o, half],
                    device_id=(sp, peers[k]), device_id_type=MESH,
                ).wait_recv()
    piece = fin.shape[4]
    for o in range(per):
        for half in range(2):
            start = (2 * o + half) * piece
            total = own_stream[:, start:start + piece]
            mixed = fin[0, o, half].astype(F32)
            for t in range(1, n_tp):
                mixed = mixed + fin[t, o, half].astype(F32)
            out_ref[:, start:start + piece] = (total + mixed).astype(BF16)

    def drain(i, carry):
        for c in range(CHUNKS):
            for half in range(2):
                d_copy(i, half, c, True).wait_send()
        return carry

    lax.fori_loop(0, n - 1, drain, 0)

    def drain_pieces(i, carry):
        for half, owner in enumerate(owners(i)):

            @pl.when(owner // per != tp)
            def _():
                f_copy(i, half, owner).wait_send()

        return carry

    lax.fori_loop(0, n, drain_pieces, 0)
    for k in range(n_tp - 1):
        p_copy(k).wait_send()
        q_copy(k).wait_send()
        y_copy(k).wait_send()


def vmem():
    return pl.BlockSpec(memory_space=pltpu.VMEM)


def hbm():
    return pl.BlockSpec(memory_space=pl.ANY)


def fused_kernel(
    n, n_tp, heads, scale, nope_ref, rope_ref, lat_ref, kr_ref, lat_gain, freq_ref, wk_in, wv_in,
    wo_ref, gain_ref, res_hbm, wu, wd,
    out_ref,
    q_ref, spin,
    wk_ref, wv_ref, xs, keys_ref, vals_ref, peak, acc, res_ref,
    far32, stream_ref, sbuf, sin, xbuf, xgot, mine, sq_mine, sqs, ys, up, down, hidden,
    hold, pieces, xin, finh, finz,
    zx_send, yx_send, x_recv, share_send, share_recv,
    wz_send, wy_send, wb_send, w_recv, b_recv, own_sem,
    s_send, s_recv, r_send, r_recv, y_send, y_recv, q_send, q_recv, f_send, f_recv,
    c_send, c_recv, e_send, e_recv, res_sem,
):
    sp = lax.axis_index("sp")
    tp = lax.axis_index("tp")
    nz = n // 2
    z, y = sp // 2, sp % 2
    x_at, core = tp // 2, tp % 2
    sib = tp + 1 - 2 * core
    far = (tp + 2) % n_tp
    across = sp + 1 - 2 * y
    mate = 2 * (z + 1 - 2 * (z % 2)) + y
    turn = 1 - 2 * (z % 2)
    inner = (z > 0) & (z < nz - 1)
    peers = [(tp + k) % n_tp for k in range(1, n_tp)]

    def half_of(zz):
        return ((zz + 1) // 2) % 2

    def z_at(k):
        return (z + turn * k + nz) % nz

    barrier = pltpu.get_barrier_semaphore()
    greet = [(2 * ((z + k) % nz) + y, tp) for k in range(1, nz)]
    greet += [(across, tp)] + [(sp, p) for p in peers] + [(mate, p) for p in peers]
    for target in greet:
        pl.semaphore_signal(barrier, inc=1, device_id=target, device_id_type=MESH)
    pl.semaphore_wait(barrier, len(greet))

    def remote(src, dst, send, recv, target):
        return pltpu.make_async_remote_copy(
            src_ref=src, dst_ref=dst, send_sem=send, recv_sem=recv,
            device_id=target, device_id_type=MESH)

    latent = wk_ref.shape[1]
    value_width = wv_ref.shape[0] // heads
    rows = nope_ref.shape[0]
    half = rows // 2
    width = stream_ref.shape[1]
    depth = wu.shape[0]
    units = up.shape[2]
    cut_u, cut_d = depth // CUTS, units // CUTS
    share_w = wd.shape[1]

    def span(r):
        return pl.ds(r * half, half)

    def zx_copy(k):
        return remote(xs.at[sp, tp], xs.at[sp, tp], zx_send.at[k - 1], x_recv.at[sp],
                      (2 * z_at(k) + y, tp))

    def yx_copy(s):
        return remote(xs.at[s, tp], xs.at[s, tp],
                      yx_send.at[s], x_recv.at[s], (across, tp))

    def x_landed(s):
        remote(xs.at[s, tp], xs.at[s, tp], yx_send.at[s], x_recv.at[s], (across, tp)).wait_recv()

    def share(s, k):
        return remote(xs.at[s, tp], xs.at[s, tp], share_send.at[s, k], share_recv.at[s, tp],
                      (sp, peers[k]))

    def share_all(s):
        for k in range(n_tp - 1):
            share(s, k).start()

    def share_wait(s):
        for k in range(n_tp - 1):
            remote(xs.at[s, tp], xs.at[s, peers[k]], share_send.at[s, k],
                   share_recv.at[s, peers[k]], (sp, peers[k])).wait_recv()

    def w_src(m, c, h):
        if m == 0:
            return wu.at[pl.ds(c * cut_u, cut_u), pl.ds(pl.multiple_of(h * units, LANES), units)]
        return wd.at[pl.ds(h * units + c * cut_d, cut_d)]

    def w_slot(m, side, s, c):
        if m == 0:
            return up.at[side, pl.ds(s * depth + c * cut_u, cut_u)]
        return down.at[s, pl.ds(side * units + c * cut_d, cut_d)]

    def wz_copy(m, k, c):
        there = z_at(k)
        return remote(w_src(m, c, half_of(there)), w_slot(m, core, sp, c),
                      wz_send.at[m, k - 1, c], w_recv.at[m, sp, c], (2 * there + y, tp))

    def wy_copy(m, s, c, first):
        slot = w_slot(m, core, s, c)
        return remote(w_src(m, c, half_of(z)) if first else slot, slot,
                      wy_send.at[m, s, c], w_recv.at[m, s, c], (across, tp))

    def wb_copy(m, s, c, first):
        slot = w_slot(m, core, s, c)
        return remote(w_src(m, c, half_of(z)) if first else slot, slot,
                      wb_send.at[m, s, c], b_recv.at[m, s, c], (sp, sib))

    def w_landed(m, s, c):
        slot = w_slot(m, core, s, c)
        remote(slot, slot, wy_send.at[m, s, c], w_recv.at[m, s, c], (across, tp)).wait_recv()

    def b_landed(m, s):
        for c in range(CUTS):
            slot = w_slot(m, 1 - core, s, c)
            remote(slot, slot, wb_send.at[m, s, c], b_recv.at[m, s, c], (sp, sib)).wait_recv()

    def own_copy(m):
        h = half_of(z)
        if m == 0:
            src = wu.at[:, pl.ds(pl.multiple_of(h * units, LANES), units)]
            dst = up.at[core, pl.ds(sp * depth, depth)]
        else:
            src = wd.at[pl.ds(h * units, units)]
            dst = down.at[sp, pl.ds(core * units, units)]
        return pltpu.make_async_copy(src, dst, own_sem.at[m])

    def z_send(m, k):
        for c in range(CUTS):
            wz_copy(m, k, c).start()

    def step_of(i):
        return i + 1

    def from_z(m, i):
        s = 2 * z_at(step_of(i)) + y
        for c in range(CUTS):
            w_landed(m, s, c)
            wy_copy(m, s, c, False).start()
            wb_copy(m, s, c, False).start()

    def from_y(m, s):
        for c in range(CUTS):
            w_landed(m, s, c)
            wb_copy(m, s, c, False).start()

    def y_origin(i):
        return 2 * z_at(step_of(i)) + 1 - y

    def grid_of(shape):
        return (lax.broadcasted_iota(jnp.int32, shape, 0),
                lax.broadcasted_iota(jnp.int32, shape, 1))

    def picks(hit):
        return jnp.where(hit, 1.0, 0.0).astype(BF16)

    turn_half = ROPE // 2

    def turned(u, span_of):
        i, j = grid_of((span_of, span_of))
        swap = picks((i // ROPE == j // ROPE) & ((i + turn_half) % ROPE == j % ROPE))
        other = jnp.dot(u, swap, preferred_element_type=F32)
        return (u.astype(F32) * spin[0, :, :span_of] + other * spin[1, :, :span_of]).astype(BF16)

    def place(out, plain, rotated):
        i, j = grid_of((heads * UNROTATED_WIDTH, heads * LANES))
        first = picks((i // UNROTATED_WIDTH == j // LANES) & (i % UNROTATED_WIDTH == j % LANES))
        i, j = grid_of((heads * ROPE, heads * LANES))
        second = picks((i // ROPE == j // LANES) & (i % ROPE + UNROTATED_WIDTH == j % LANES))
        out[...] = (
            jnp.dot(plain[...], first, preferred_element_type=F32)
            + jnp.dot(rotated, second, preferred_element_type=F32)).astype(BF16)

    def flipped(u):
        i, j = grid_of((u.shape[1], u.shape[1]))
        return lax.dot_general(picks(i == j), u, NT, preferred_element_type=F32).astype(BF16)

    line, lane = grid_of((rows, LANES))
    phases = (sp * rows + line).astype(F32) * freq_ref[...]
    spin[0] = jnp.cos(phases)
    sine = jnp.sin(phases)
    spin[1] = jnp.where(lane % ROPE < turn_half, -sine, sine)
    lat = flipped(rms_scale(lat_ref[...].astype(F32), lat_gain[...]).astype(BF16))
    rot = flipped(turned(kr_ref[...], ROPE))
    chunk = rows // n_tp
    for t in range(n_tp):
        xs[sp, t, :latent] = lat[:, t * chunk:(t + 1) * chunk]
        xs[sp, t, latent:] = rot[:, t * chunk:(t + 1) * chunk]

    for k in range(1, nz):
        zx_copy(k).start()
    yx_copy(sp).start()
    for k in range(1, nz):
        z_send(0, k)

    @pl.when(inner)
    def _():
        for k in range(1, nz):
            z_send(1, k)

    for c in range(CUTS):
        wy_copy(0, sp, c, True).start()
    for m in range(2):
        own_copy(m).start()
    for m in range(2):
        for c in range(CUTS):
            wb_copy(m, sp, c, True).start()
    res_copy = pltpu.make_async_copy(
        res_hbm.at[:, pl.ds(pl.multiple_of(tp * width, LANES), width)], res_ref, res_sem)
    res_copy.start()
    wk_ref[...] = jnp.transpose(wk_in[...].astype(F32)).astype(BF16)
    wv_ref[...] = jnp.transpose(wv_in[...].astype(F32)).astype(BF16)
    peak[...] = jnp.full(peak.shape, -1e30, F32)
    acc[...] = jnp.zeros(acc.shape, F32)
    place(q_ref, nope_ref, turned(rope_ref[...], LANES))

    def project_keys(s):
        block = jnp.concatenate([xs[s, t] for t in range(n_tp)], axis=1)
        lat = block[:latent]
        rot = block[latent:]
        count = block.shape[1]
        k_all = jnp.dot(wk_ref[...], lat, preferred_element_type=F32).astype(BF16)
        v_all = jnp.dot(wv_ref[...], lat, preferred_element_type=F32).astype(BF16)
        k_pad = jnp.zeros((LANES - UNROTATED_WIDTH - rot.shape[0], count), BF16)
        ones = jnp.ones((16, count), BF16)
        v_pad = jnp.zeros((LANES - value_width - 16, count), BF16)
        for h in range(heads):
            keys_ref[s, h] = jnp.concatenate(
                [k_all[h * UNROTATED_WIDTH:(h + 1) * UNROTATED_WIDTH], rot, k_pad], axis=0)
            vals_ref[s, h] = jnp.concatenate(
                [v_all[h * value_width:(h + 1) * value_width], ones, v_pad], axis=0)

    def attend(s, r, size):
        lines = pl.ds(r * half, size)
        for h in range(heads):
            score = jnp.dot(q_ref[lines, h * LANES:(h + 1) * LANES], keys_ref[s, h],
                            preferred_element_type=F32)
            old = peak[h, lines]
            new = jnp.maximum(old, jnp.max(score, axis=1, keepdims=True))
            p = jnp.exp2((score - new) * scale).astype(BF16)
            acc[h, lines] = acc[h, lines] * jnp.exp2((old - new) * scale) + lax.dot_general(
                p, vals_ref[s, h], NT, preferred_element_type=F32)
            peak[h, lines] = new

    def block_at(b):
        flip = (b - 2) // (nz - 1)
        off = (b - 2) % (nz - 1) + 1
        there = 2 * ((z + off) % nz) + (y + flip) % 2
        return there

    def s_copy(r):
        return remote(sbuf.at[r], sin.at[r], s_send.at[r], s_recv.at[r], (sp, sib))

    def r_copy(r):
        return remote(xbuf.at[r], xgot.at[r], r_send.at[r], r_recv.at[r], (sp, far))

    def project(r):
        group = []
        for h in range(heads):
            a = acc[h, span(r)]
            group.append((a[:, :value_width] / a[:, value_width:value_width + 1]).astype(BF16))
        attended = jnp.concatenate(group, axis=1)

        def quarter(t):
            return jnp.dot(attended, wo_ref[:, pl.ds(pl.multiple_of(t * width, LANES), width)],
                           preferred_element_type=F32)

        sbuf[r, 0] = quarter(sib).astype(BF16)
        sbuf[r, 1] = quarter((sib + 2) % n_tp).astype(BF16)
        s_copy(r).start()
        far32[span(r)] = quarter(far)
        stream_ref[span(r)] = quarter(tp)

    def relay(r):
        s_copy(r).wait_recv()
        xbuf[r] = (far32[span(r)] + sin[r, 1].astype(F32)).astype(BF16)
        r_copy(r).start()

    home_far = 2 * (1 - x_at)

    def columns(t):
        return pl.ds(pl.multiple_of(t * width, LANES), width)

    def y_copy(r, which):
        target = ((sp, sib), (sp, home_far), (mate, 2 * x_at + 1))[which]
        return remote(mine.at[span(r)], ys.at[span(r), columns(tp)],
                      y_send.at[r, which], y_recv.at[r, tp], target)

    def q_copy(r, which):
        target = ((sp, sib), (sp, home_far), (mate, 2 * x_at + 1), (mate, home_far + 1))[which]
        return remote(sq_mine.at[r], sqs.at[r, tp], q_send.at[r, which], q_recv.at[r, tp], target)

    def f_copy(r, i):
        t = 2 * x_at + i
        return remote(ys.at[span(r), columns(t)], ys.at[span(r), columns(t)],
                      f_send.at[r, i], y_recv.at[r, t], (sp, home_far + 1))

    def y_wait(r, t):
        remote(mine.at[span(r)], ys.at[span(r), columns(t)],
               y_send.at[r, 1], y_recv.at[r, t], (sp, home_far)).wait_recv()

    def q_wait(r, t):
        remote(sq_mine.at[r], sqs.at[r, t], q_send.at[r, 1], q_recv.at[r, t],
               (sp, home_far)).wait_recv()

    def settle(r):
        r_copy(r).wait_recv()
        stream = stream_ref[span(r)] + sin[r, 0].astype(F32) + xgot[r].astype(F32)
        stream = stream + res_ref[span(r)].astype(F32)
        stream_ref[span(r)] = stream
        shard = (stream * gain_ref[tp]).astype(BF16)
        mine[span(r)] = shard
        total = jnp.sum(stream * stream, axis=1, keepdims=True)
        squares = jnp.transpose(jnp.broadcast_to(total, (half, LANES)))[:8]
        sq_mine[r] = squares

        @pl.when(core == 0)
        def _():
            ys[span(r), columns(tp)] = shard
            sqs[r, tp] = squares

        q_copy(r, 2).start()
        y_copy(r, 2).start()
        q_copy(r, 3).start()
        q_copy(r, 1).start()
        y_copy(r, 1).start()

        @pl.when(core == 1)
        def _():
            q_copy(r, 0).start()
            y_copy(r, 0).start()

    def pass_on(r):
        @pl.when(core == 1)
        def _():
            for i in range(2):
                y_wait(r, 2 * x_at + i)
                f_copy(r, i).start()

    def gathered(r):
        @pl.when(core == 1)
        def _():
            for i in range(2):
                y_wait(r, home_far + i)
            for t in range(n_tp):
                q_wait(r, t)

        @pl.when(core == 0)
        def _():
            for t in peers:
                y_wait(r, t)
                q_wait(r, t)

    project_keys(sp)
    attend(sp, 0, half)
    x_landed(across)
    share_all(across)
    attend(sp, 1, half)
    for off in range(1, nz):
        s = 2 * ((z + off) % nz) + y
        x_landed(s)
        yx_copy(s).start()
        share_all(s)
    for c in range(CUTS):
        wy_copy(1, sp, c, True).start()

    split = n // 2

    def first_blocks(b, carry):
        s = jnp.where(b == 1, across, block_at(b))
        share_wait(s)
        project_keys(s)
        attend(s, 0, rows)

        @pl.when(b == 2)
        def _():
            for off in range(1, nz):
                there = 2 * ((z + off) % nz) + 1 - y
                x_landed(there)
                share_all(there)
            from_z(0, 0)

        return carry

    def second_blocks(b, carry):
        s = block_at(b)
        share_wait(s)
        project_keys(s)
        attend(s, 0, half)

        @pl.when(b == n - 1)
        def _():
            from_y(0, across)
            from_z(0, 1)

        return carry

    def third_blocks(b, carry):
        attend(block_at(b), 1, half)

        @pl.when(b == split)
        def _():
            relay(0)

        @pl.when(b == split + 1)
        def _():
            from_y(0, y_origin(0))

        return carry

    def late_sends(k, c0, c1):
        @pl.when(z * (nz - 1 - z) == 0)
        def _():
            for c in range(c0, c1):
                wz_copy(1, k, c).start()

    lax.fori_loop(1, split, first_blocks, 0)
    lax.fori_loop(split, n, second_blocks, 0)
    res_copy.wait()
    project(0)
    lax.fori_loop(split, n, third_blocks, 0)
    project(1)
    settle(0)
    late_sends(1, 0, CUTS // 2)
    relay(1)
    settle(1)
    late_sends(1, CUTS // 2, CUTS)
    for k in range(2, nz):
        late_sends(k, 0, CUTS)
    for i in range(2, nz - 1):
        from_z(0, i)
    pass_on(0)
    from_y(0, y_origin(1))
    pass_on(1)
    for i in range(2, nz - 1):
        from_y(0, y_origin(i))
    from_z(1, 0)
    own_copy(0).wait()
    for s in range(n):
        b_landed(0, s)
    gathered(0)
    gathered(1)

    factors = []
    for r in range(2):
        squares = sqs[r, 0]
        for t in range(1, n_tp):
            squares = squares + sqs[r, t]
        squares = jnp.concatenate([squares] * (LANES // 8), axis=0)
        factors.append(jnp.transpose(squares)[:, :1])
    factor = lax.rsqrt(jnp.concatenate(factors, axis=0) / (width * n_tp) + epsilon)
    tile = math.gcd(units, 512)
    tiles = units // tile

    def up_step(i, carry):
        within = pl.ds(pl.multiple_of((i % tiles) * tile, tile), tile)
        total = jnp.dot(ys[...], up[i // tiles, :, within], preferred_element_type=F32)
        total = jnp.maximum(total, 0.0) * factor
        hidden[:, pl.ds(pl.multiple_of(i * tile, tile), tile)] = (total * total).astype(BF16)

        @pl.when(i == 1)
        def _():
            from_z(1, 1)

        return carry

    lax.fori_loop(0, 2 * tiles, up_step, 0)

    per = n // n_tp

    def order(j):
        i = (j - 2) // 2
        there = 2 * z_at(step_of(i)) + (y + j) % 2
        return jnp.where(j == 0, sp, jnp.where(j == 1, across, there))

    def c_copy(s):
        return remote(pieces.at[s], xin.at[s % nz], c_send.at[s], c_recv.at[s % nz], (sp, far))

    def e_copy(s):
        return remote(pieces.at[s], finh.at[s % per], e_send.at[s], e_recv.at[0, s % per],
                      (sp, s // per))

    def g_copy(s):
        return remote(pieces.at[s], finz.at[s % per], e_send.at[s], e_recv.at[1, s % per],
                      (mate, s // per))

    def owner_is_here(s):
        return s // nz == x_at

    def finish(s):
        @pl.when(owner_is_here(s))
        def _():
            c_copy(s).wait_recv()
            value = (hold[s % nz] + xin[s % nz].astype(F32)).astype(BF16)

            @pl.when(core == 1)
            def _():
                pieces[s] = value
                g_copy(s).start()

            @pl.when(core == 0)
            def _():
                @pl.when(s // per == tp)
                def _():
                    finh[s % per] = value

                @pl.when(s // per != tp)
                def _():
                    pieces[s] = value
                    e_copy(s).start()

    own_copy(1).wait()

    def down_step(j, carry):
        s = order(j)
        i = (j - 2) // 2

        @pl.when(j % 2 == 1)
        def _():
            from_y(1, s)

        @pl.when((j % 2 == 0) & (j >= 4) & (j < n - 2))
        def _():
            from_z(1, i + 1)

        b_landed(1, s)
        term = jnp.dot(hidden[...], down[s], preferred_element_type=F32)

        @pl.when(owner_is_here(s))
        def _():
            hold[s % nz] = term

        @pl.when(s // nz != x_at)
        def _():
            pieces[s] = term.astype(BF16)
            c_copy(s).start()

        @pl.when(j >= LAG)
        def _():
            finish(order(j - LAG))

        return carry

    lax.fori_loop(0, n, down_step, 0)

    def last_step(j, carry):
        finish(order(j))
        return carry

    lax.fori_loop(n - LAG, n, last_step, 0)

    for o in range(per):
        s = tp * per + o
        g_copy(s).wait_recv()

        @pl.when(core == 1)
        def _():
            e_copy(s).wait_recv()

        cols = slice(o * share_w, (o + 1) * share_w)
        out_ref[:, cols] = (
            stream_ref[:, cols] + (finh[o].astype(F32) + finz[o].astype(F32))).astype(BF16)

    for k in range(1, nz):
        zx_copy(k).wait_send()
        for m in range(2):
            for c in range(CUTS):
                wz_copy(m, k, c).wait_send()
    yx_copy(sp).wait_send()
    for k in range(n_tp - 1):
        share(across, k).wait_send()
    for off in range(1, nz):
        s = 2 * ((z + off) % nz) + y
        yx_copy(s).wait_send()
        for k in range(n_tp - 1):
            share(s, k).wait_send()
            share(2 * ((z + off) % nz) + 1 - y, k).wait_send()
    for off in range(nz):
        s = 2 * ((z + off) % nz) + y
        for m in range(2):
            for c in range(CUTS):
                wy_copy(m, s, c, False).wait_send()

    def drain(s, carry):
        for m in range(2):
            for c in range(CUTS):
                wb_copy(m, s, c, False).wait_send()

        @pl.when(s // nz != x_at)
        def _():
            c_copy(s).wait_send()

        @pl.when(owner_is_here(s) & ((core == 1) | (s // per != tp)))
        def _():
            g_copy(s).wait_send()

        return carry

    lax.fori_loop(0, n, drain, 0)
    for r in range(2):
        s_copy(r).wait_send()
        r_copy(r).wait_send()
        for which in range(1, 3):
            y_copy(r, which).wait_send()
        for which in range(1, 4):
            q_copy(r, which).wait_send()

        @pl.when(core == 1)
        def _():
            y_copy(r, 0).wait_send()
            q_copy(r, 0).wait_send()
            for i in range(2):
                f_copy(r, i).wait_send()


def fused(
    n, n_tp, heads, scale, queries, rope_queries, latents, rope_keys, latent_gain,
    key_up, value_up, w_out, gain, residual, w_up, w_down,
):
    rows, model = residual.shape
    depth, units = w_up.shape[0], w_up.shape[1] // 2
    share_w = w_down.shape[1]
    width = model // n_tp
    wide = latents.shape[1] + ROPE
    rates = np.arange(0, ROPE, 2, dtype=np.float32) / np.float32(ROPE)
    rates = np.float32(1.0) / np.float32(rope_base) ** rates
    rates = np.tile(rates, LANES // rates.shape[0])[None, :]
    half, nz, per = rows // 2, n // 2, n // n_tp
    dma = pltpu.SemaphoreType.DMA
    return pl.pallas_call(
        functools.partial(fused_kernel, n, n_tp, heads, scale),
        out_shape=jax.ShapeDtypeStruct((rows, width), BF16),
        in_specs=[vmem()] * 10 + [hbm()] * 3,
        out_specs=vmem(),
        scratch_shapes=[
            pltpu.VMEM((rows, heads * LANES), BF16),
            pltpu.VMEM((2, rows, LANES), F32),
            pltpu.VMEM(key_up.shape[::-1], BF16),
            pltpu.VMEM(value_up.shape[::-1], BF16),
            pltpu.VMEM((n, n_tp, wide, rows // n_tp), BF16),
            pltpu.VMEM((n, heads, LANES, rows), BF16),
            pltpu.VMEM((n, heads, LANES, rows), BF16),
            pltpu.VMEM((heads, rows, 1), F32),
            pltpu.VMEM((heads, rows, LANES), F32),
            pltpu.VMEM((rows, width), BF16),
            pltpu.VMEM((rows, width), F32),
            pltpu.VMEM((rows, width), F32),
            pltpu.VMEM((2, 2, half, width), BF16),
            pltpu.VMEM((2, 2, half, width), BF16),
            pltpu.VMEM((2, half, width), BF16),
            pltpu.VMEM((2, half, width), BF16),
            pltpu.VMEM((rows, width), BF16),
            pltpu.VMEM((2, 8, half), F32),
            pltpu.VMEM((2, n_tp, 8, half), F32),
            pltpu.VMEM((rows, model), BF16),
            pltpu.VMEM((2, model, units), BF16),
            pltpu.VMEM((n, 2 * units, share_w), BF16),
            pltpu.VMEM((rows, 2 * units), BF16),
            pltpu.VMEM((nz, rows, share_w), F32),
            pltpu.VMEM((n, rows, share_w), BF16),
            pltpu.VMEM((nz, rows, share_w), BF16),
            pltpu.VMEM((per, rows, share_w), BF16),
            pltpu.VMEM((per, rows, share_w), BF16),
            dma((nz - 1,)), dma((n,)), dma((n,)), dma((n, n_tp - 1)), dma((n, n_tp)),
            dma((2, nz - 1, CUTS)), dma((2, n, CUTS)), dma((2, n, CUTS)),
            dma((2, n, CUTS)), dma((2, n, CUTS)), dma((2,)),
            dma((2,)), dma((2,)), dma((2,)), dma((2,)),
            dma((2, 3)), dma((2, n_tp)), dma((2, 4)), dma((2, n_tp)),
            dma((2, 2)), dma((2, 2)),
            dma((n,)), dma((nz,)), dma((n,)), dma((2, per)), dma,
        ],
        compiler_params=pltpu.CompilerParams(
            collective_id=2, has_side_effects=True, vmem_limit_bytes=62 * 2**20),
        name="layer",
    )(
        queries, rope_queries, latents, rope_keys, latent_gain[None, :], jnp.asarray(rates),
        key_up, value_up, w_out, gain, residual, w_up, w_down,
    )


def on_device(
    n,
    n_tp,
    residual_in,
    queries_nope,
    queries_rope,
    latents,
    rope_keys,
    latent_norm_gain,
    key_up_weight,
    value_up_weight,
    w_out,
    norm_gain,
    w_up,
    w_down,
):
    rows, model = residual_in.shape
    heads = key_up_weight.shape[1] // UNROTATED_WIDTH
    value_width = value_up_weight.shape[1] // heads
    width = model // n_tp
    depth, units = w_up.shape
    scale = math.log2(math.e) / math.sqrt(UNROTATED_WIDTH + ROPE)
    lined = depth % (16 * CUTS) == 0 and w_down.shape[1] % LANES == 0 and rows % 512 == 0
    fits = heads * ROPE == LANES and n % 4 == 0 and n > 4 and n % (2 * n_tp) == 0
    if fits and lined and n_tp == 4:
        return fused(
            n, n_tp, heads, scale, queries_nope, queries_rope, latents, rope_keys,
            latent_norm_gain, key_up_weight, value_up_weight, w_out,
            norm_gain.reshape(n_tp, 1, width), residual_in, w_up, w_down)
    positions = lax.axis_index("sp") * rows + jnp.arange(rows, dtype=jnp.int32)
    phases = rope_phases(positions, ROPE)
    q_rot = rotate(
        queries_rope.astype(F32).reshape(rows, heads, ROPE), phases[:, None, :]
    ).astype(BF16)
    queries = jnp.concatenate(
        [
            queries_nope.reshape(rows, heads, UNROTATED_WIDTH),
            q_rot,
            jnp.zeros((rows, heads, LANES - UNROTATED_WIDTH - ROPE), BF16),
        ],
        axis=2,
    ).reshape(rows, heads * LANES)
    lat_norm = rms_scale(latents.astype(F32), latent_norm_gain).astype(BF16)
    key_rot = rotate(rope_keys.astype(F32), phases).astype(BF16)
    x = jnp.concatenate([lat_norm, key_rot], axis=1)
    wide = x.shape[1]
    x = jnp.transpose(x.reshape(n_tp, rows // n_tp, wide), (0, 2, 1))

    dma = pltpu.SemaphoreType.DMA
    part, full = pl.pallas_call(
        functools.partial(
            attention_kernel, n, n_tp, heads, scale),
        out_shape=(
            jax.ShapeDtypeStruct((n_tp, rows, width), BF16),
            jax.ShapeDtypeStruct((n, 2, CHUNKS, depth // 2 // CHUNKS, units), BF16),
        ),
        in_specs=[vmem()] * 5 + [hbm()],
        out_specs=(vmem(), hbm()),
        scratch_shapes=[
            pltpu.VMEM(key_up_weight.shape[::-1], BF16),
            pltpu.VMEM(value_up_weight.shape[::-1], BF16),
            pltpu.VMEM((n, n_tp, wide, rows // n_tp), BF16),
            pltpu.VMEM((heads, rows, 1), F32),
            pltpu.VMEM((heads, rows, LANES), F32),
            dma((n - 1,)), dma((n - 1,)),
            dma((n, n_tp - 1)), dma((n, n_tp - 1)),
            dma((n - 1, 2, CHUNKS)), dma((n - 1, 2, CHUNKS)), dma,
        ],
        compiler_params=pltpu.CompilerParams(
            collective_id=0, has_side_effects=True, vmem_limit_bytes=56 * 2**20),
        name="attend",
    )(
        queries, x, key_up_weight, value_up_weight,
        w_out, w_up.reshape(2, CHUNKS, depth // 2 // CHUNKS, units),
    )

    hidden_units, share = w_down.shape
    narrow = (share // 2) % LANES != 0
    if narrow:
        down_in = jnp.transpose(w_down.reshape(hidden_units, 2, share // 2), (1, 2, 0))
        half_shape = (share // 2, hidden_units)
    else:
        down_in = w_down
        half_shape = (hidden_units, share // 2)
    per = n // n_tp
    return pl.pallas_call(
        functools.partial(feed_kernel, n, n_tp, narrow),
        out_shape=jax.ShapeDtypeStruct((rows, width), BF16),
        in_specs=[vmem(), hbm(), vmem(), hbm(), hbm()],
        out_specs=vmem(),
        scratch_shapes=[
            pltpu.VMEM((rows, width), BF16),
            pltpu.VMEM((model, units), BF16),
            pltpu.VMEM((n, 2) + half_shape, BF16),
            pltpu.VMEM((n_tp - 1, rows, width), BF16),
            pltpu.VMEM((n_tp, rows, width), BF16),
            pltpu.VMEM((n_tp, 8, rows), F32),
            pltpu.VMEM((rows, width), F32),
            pltpu.VMEM((rows, units), BF16),
            pltpu.VMEM((n, 2, rows, share // 2), BF16),
            pltpu.VMEM((n_tp, per, 2, rows, share // 2), BF16),
            dma((n - 1, 2, CHUNKS)), dma((n - 1, 2, CHUNKS)),
            dma((n_tp - 1,)), dma((n_tp - 1,)),
            dma((n_tp - 1,)), dma((n_tp - 1,)),
            dma((n_tp - 1,)), dma((n_tp - 1,)),
            dma((n, 2)), dma((n_tp, per, 2)),
            dma((4,)),
        ],
        compiler_params=pltpu.CompilerParams(
            collective_id=1, has_side_effects=True, vmem_limit_bytes=60 * 2**20),
        name="feed",
    )(part, residual_in, norm_gain.reshape(n_tp, 1, width), full.reshape(model, units), down_in)


def solution(mesh):
    in_specs = (
        P("sp", None),
        P("sp", "tp"),
        P("sp", "tp"),
        P("sp", None),
        P("sp", None),
        P(),
        P(None, "tp"),
        P(None, "tp"),
        P("tp", None),
        P(),
        P("sp", "tp"),
        P("tp", "sp"),
    )
    out_specs = P("sp", "tp")
    return jax.shard_map(
        functools.partial(on_device, mesh.shape["sp"], mesh.shape["tp"]),
        mesh=mesh, in_specs=in_specs, out_specs=out_specs, check_vma=False,
    )
```

```python
import functools
import math

import jax
import jax.numpy as jnp
import numpy as np
from jax import lax
from jax.experimental import pallas as pl
from jax.experimental.pallas import tpu as pltpu
from jax.sharding import PartitionSpec as P

UNROTATED_WIDTH = 64
ROPE = 32
LANES = 128
CHUNKS = 4
CUTS = 2
LAG = 5

rope_base = 10000.0
epsilon = 1e-06
F32 = jnp.float32
BF16 = jnp.bfloat16
MESH = pl.DeviceIdType.MESH
NT = (((1,), (1,)), ((), ()))


def rotate(vectors, phases):
    half_width = vectors.shape[-1] // 2
    first_half = vectors[..., :half_width]
    second_half = vectors[..., half_width:]
    cosine = jnp.cos(phases)
    sine = jnp.sin(phases)
    return jnp.concatenate(
        [first_half * cosine - second_half * sine, second_half * cosine + first_half * sine],
        axis=-1,
    )


def rope_phases(positions, width):
    inverse = 1.0 / rope_base ** (jnp.arange(0, width, 2, dtype=jnp.float32) / width)
    return positions.astype(jnp.float32)[:, None] * inverse[None, :]


def rms_scale(vectors, gain_vec):
    return (
        vectors
        * lax.rsqrt(jnp.mean(vectors * vectors, axis=-1, keepdims=True) + epsilon)
        * gain_vec
    )


def ring_of(index, n):
    return index // 2 + (index % 2) * (n - 1 - 2 * (index // 2))


def index_of(place, n):
    return 2 * place + (place // (n // 2)) * (2 * n - 1 - 4 * place)


def ring_ids(n):
    place = ring_of(lax.axis_index("sp"), n)

    def at(offset):
        return index_of((place + offset + 2 * n) % n, n)

    return at


def attention_kernel(
    n, n_tp, heads, scale, q_ref, x_ref, wk_in, wv_in, wo_ref, wu_ref,
    part_ref, full_ref,
    wk_ref, wv_ref, xs, peak, acc, xsend, xrecv, ssend, srecv, wsend, wrecv, own_sem,
):
    at = ring_ids(n)
    tp = lax.axis_index("tp")
    me = lax.axis_index("sp")
    to = ((at(1), tp), (at(-1), tp))
    peers = [(tp + k) % n_tp for k in range(1, n_tp)]
    onward = (at(1 - 2 * (tp % 2)), tp)
    barrier = pltpu.get_barrier_semaphore()
    for target in list(to) + [(me, p) for p in peers]:
        pl.semaphore_signal(barrier, inc=1, device_id=target, device_id_type=MESH)
    pl.semaphore_wait(barrier, 2 + n_tp - 1)

    latent = wk_ref.shape[1]
    value_width = wv_ref.shape[0] // heads

    def x_copy(step, src):
        return pltpu.make_async_remote_copy(
            src_ref=src, dst_ref=xs.at[step + 1, tp],
            send_sem=xsend.at[step], recv_sem=xrecv.at[step],
            device_id=onward, device_id_type=MESH,
        )

    def share(step, k):
        return pltpu.make_async_remote_copy(
            src_ref=xs.at[step, tp], dst_ref=xs.at[step, tp],
            send_sem=ssend.at[step, k], recv_sem=srecv.at[step, k],
            device_id=(me, peers[k]), device_id_type=MESH,
        )

    def share_wait(step):
        for k in range(n_tp - 1):
            pltpu.make_async_remote_copy(
                src_ref=xs.at[step, tp], dst_ref=xs.at[step, (tp + n_tp - 1 - k) % n_tp],
                send_sem=ssend.at[step, k], recv_sem=srecv.at[step, k],
                device_id=(me, peers[k]), device_id_type=MESH,
            ).wait_recv()

    def w_copy(step, half, c, first):
        owner = at(-step) if half == 0 else at(step)
        return pltpu.make_async_remote_copy(
            src_ref=wu_ref.at[half, c] if first else full_ref.at[owner, half, c],
            dst_ref=full_ref.at[owner, half, c],
            send_sem=wsend.at[step, half, c], recv_sem=wrecv.at[step, half, c],
            device_id=to[half], device_id_type=MESH,
        )

    x_copy(0, x_ref.at[tp]).start()
    for c in range(CHUNKS):
        for half in range(2):
            w_copy(0, half, c, True).start()
    own = pltpu.make_async_copy(wu_ref, full_ref.at[me], own_sem)
    own.start()
    wk_ref[...] = jnp.transpose(wk_in[...].astype(F32)).astype(BF16)
    wv_ref[...] = jnp.transpose(wv_in[...].astype(F32)).astype(BF16)
    peak[...] = jnp.full(peak.shape, -1e30, F32)
    acc[...] = jnp.zeros(acc.shape, F32)

    def attend(blocks):
        block = jnp.concatenate(blocks, axis=1)
        lat = block[:latent]
        rot = block[latent:]
        keys = block.shape[1]
        k_all = jnp.dot(wk_ref[...], lat, preferred_element_type=F32).astype(BF16)
        v_all = jnp.dot(wv_ref[...], lat, preferred_element_type=F32).astype(BF16)
        k_pad = jnp.zeros((LANES - UNROTATED_WIDTH - rot.shape[0], keys), BF16)
        ones = jnp.ones((16, keys), BF16)
        v_pad = jnp.zeros((LANES - value_width - 16, keys), BF16)
        for h in range(heads):
            k_h = jnp.concatenate(
                [k_all[h * UNROTATED_WIDTH:(h + 1) * UNROTATED_WIDTH], rot, k_pad], axis=0)
            v_h = jnp.concatenate(
                [v_all[h * value_width:(h + 1) * value_width], ones, v_pad], axis=0)
            s = jnp.dot(q_ref[:, h * LANES:(h + 1) * LANES], k_h, preferred_element_type=F32)
            old = peak[h]
            new = jnp.maximum(old, jnp.max(s, axis=1, keepdims=True))
            p = jnp.exp2((s - new) * scale).astype(BF16)
            acc[h] = acc[h] * jnp.exp2((old - new) * scale) + lax.dot_general(
                p, v_h, NT, preferred_element_type=F32)
            peak[h] = new

    def turn(i, carry):
        x_copy(i - 1, x_ref.at[tp]).wait_recv()
        x_copy(i, xs.at[i, tp]).start()
        for k in range(n_tp - 1):
            share(i, k).start()
        for c in range(CHUNKS):
            for half in range(2):
                w_copy(i - 1, half, c, True).wait_recv()
                w_copy(i, half, c, False).start()

        @pl.when(i > 1)
        def _():
            share_wait(i - 1)
            attend([xs[i - 1, t] for t in range(n_tp)])

        return carry

    attend([x_ref[t] for t in range(n_tp)])
    lax.fori_loop(1, n - 1, turn, 0)
    x_copy(n - 2, x_ref.at[tp]).wait_recv()
    for k in range(n_tp - 1):
        share(n - 1, k).start()

    def last(i, carry):
        share_wait(i)
        attend([xs[i, t] for t in range(n_tp)])
        return carry

    lax.fori_loop(n - 2, n, last, 0)

    width = part_ref.shape[2]
    group = []
    for h in range(heads):
        a = acc[h]
        group.append((a[:, :value_width] / a[:, value_width:value_width + 1]).astype(BF16))
    attended = jnp.concatenate(group, axis=1)
    for j in range(part_ref.shape[0]):
        part_ref[j] = jnp.dot(
            attended, wo_ref[:, j * width:(j + 1) * width], preferred_element_type=F32
        ).astype(BF16)

    own.wait()
    for c in range(CHUNKS):
        for half in range(2):
            w_copy(n - 2, half, c, True).wait_recv()

    def drain(i, carry):
        x_copy(i, x_ref.at[tp]).wait_send()
        for k in range(n_tp - 1):
            share(i + 1, k).wait_send()
        for c in range(CHUNKS):
            for half in range(2):
                w_copy(i, half, c, True).wait_send()
        return carry

    lax.fori_loop(0, n - 1, drain, 0)


def feed_kernel(
    n, n_tp, narrow, part_ref, res_hbm, gain_ref, up_hbm, wd_hbm,
    out_ref,
    res_ref, up, down, parts, ys, sq, own_stream, hidden, pieces, fin,
    dsend, drecv, psend, precv, ysend, yrecv, qsend, qrecv, fsend, frecv, local,
):
    at = ring_ids(n)
    tp = lax.axis_index("tp")
    sp = lax.axis_index("sp")
    to = ((at(1), tp), (at(-1), tp))
    peers = [(tp + k) % n_tp for k in range(1, n_tp)]
    barrier = pltpu.get_barrier_semaphore()
    for target in list(to) + [(sp, p) for p in peers]:
        pl.semaphore_signal(barrier, inc=1, device_id=target, device_id_type=MESH)
    pl.semaphore_wait(barrier, 2 + n_tp - 1)

    rows, width = res_ref.shape
    per = n // n_tp

    lines = down.shape[2] // CHUNKS

    def own_half(half):
        if narrow:
            return wd_hbm.at[half]
        return wd_hbm.at[:, half * down.shape[3]:(half + 1) * down.shape[3]]

    def d_copy(step, half, c, first):
        span = pl.ds(c * lines, lines)
        if not first:
            src = down.at[step, half, span]
        elif narrow:
            src = wd_hbm.at[half, span]
        else:
            src = wd_hbm.at[span, half * down.shape[3]:(half + 1) * down.shape[3]]
        return pltpu.make_async_remote_copy(
            src_ref=src, dst_ref=down.at[step + 1, half, span],
            send_sem=dsend.at[step, half, c], recv_sem=drecv.at[step, half, c],
            device_id=to[half], device_id_type=MESH,
        )

    def p_copy(k):
        peer = peers[k]
        return pltpu.make_async_remote_copy(
            src_ref=part_ref.at[peer], dst_ref=parts.at[k],
            send_sem=psend.at[k], recv_sem=precv.at[k],
            device_id=(sp, peer), device_id_type=MESH,
        )

    def y_copy(k):
        return pltpu.make_async_remote_copy(
            src_ref=ys.at[tp], dst_ref=ys.at[tp],
            send_sem=ysend.at[k], recv_sem=yrecv.at[k],
            device_id=(sp, peers[k]), device_id_type=MESH,
        )

    def q_copy(k):
        return pltpu.make_async_remote_copy(
            src_ref=sq.at[0], dst_ref=sq.at[k + 1],
            send_sem=qsend.at[k], recv_sem=qrecv.at[k],
            device_id=(sp, peers[k]), device_id_type=MESH,
        )

    def landed(step, c):
        for half in range(2):
            d_copy(step, half, c, True).wait_recv()

    def event(step, c):
        landed(step - 1, c)
        for half in range(2):
            d_copy(step, half, c, False).start()

    def events(first, last):
        for tick in range(first, last):
            event(1 + tick // CHUNKS, tick % CHUNKS)

    for c in range(CHUNKS):
        for half in range(2):
            d_copy(0, half, c, True).start()
    for k in range(n_tp - 1):
        p_copy(k).start()
    loads = [
        pltpu.make_async_copy(
            res_hbm.at[:, pl.ds(pl.multiple_of(tp * width, LANES), width)], res_ref, local.at[0]),
        pltpu.make_async_copy(up_hbm, up, local.at[1]),
        pltpu.make_async_copy(own_half(0), down.at[0, 0], local.at[2]),
        pltpu.make_async_copy(own_half(1), down.at[0, 1], local.at[3]),
    ]
    for load in loads:
        load.start()

    early = 4
    events(0, 6)
    for k in range(n_tp - 1):
        p_copy(k).wait_recv()
    loads[0].wait()
    stream = part_ref[tp].astype(F32)
    for k in range(n_tp - 1):
        stream = stream + parts[k].astype(F32)
    stream = stream + res_ref[...].astype(F32)
    own_stream[...] = stream
    ys[tp] = (stream * gain_ref[tp]).astype(BF16)
    total = jnp.sum(stream * stream, axis=1, keepdims=True)
    sq[0] = jnp.transpose(jnp.broadcast_to(total, (rows, LANES)))[:8]
    for k in range(n_tp - 1):
        q_copy(k).start()
        y_copy(k).start()
    events(6, 12)
    for k in range(n_tp - 1):
        q_copy(k).wait_recv()
    for k in range(n_tp - 1):
        pltpu.make_async_remote_copy(
            src_ref=ys.at[tp], dst_ref=ys.at[(tp + n_tp - 1 - k) % n_tp],
            send_sem=ysend.at[k], recv_sem=yrecv.at[k],
            device_id=(sp, peers[k]), device_id_type=MESH,
        ).wait_recv()
    squares = sq[0]
    for k in range(1, n_tp):
        squares = squares + sq[k]
    squares = jnp.concatenate([squares] * (LANES // 8), axis=0)
    factor = lax.rsqrt(jnp.transpose(squares)[:, :1] / (width * n_tp) + epsilon)
    loads[1].wait()
    units = hidden.shape[1]
    tile = math.gcd(units, 512)

    def up_step(c, carry):
        columns = pl.ds(pl.multiple_of(c * tile, tile), tile)
        total = jnp.dot(ys[0], up[:width, columns], preferred_element_type=F32)
        for t in range(1, n_tp):
            total = total + jnp.dot(
                ys[t], up[t * width:(t + 1) * width, columns], preferred_element_type=F32)
        total = jnp.maximum(total, 0.0) * factor
        hidden[:, columns] = (total * total).astype(BF16)

        @pl.when(c < CHUNKS)
        def _():
            event(early, c)

        return carry

    lax.fori_loop(0, units // tile, up_step, 0)

    def owners(i):
        return at(-i), at(i)

    def f_copy(i, half, owner):
        return pltpu.make_async_remote_copy(
            src_ref=pieces.at[i, half],
            dst_ref=fin.at[tp, owner % per, half],
            send_sem=fsend.at[i, half], recv_sem=frecv.at[tp, owner % per, half],
            device_id=(sp, owner // per), device_id_type=MESH,
        )

    def down_block(i, left, right):
        if narrow:
            block = jnp.concatenate([left, right], axis=0)
            half_width = left.shape[0]
            term = lax.dot_general(hidden[...], block, NT, preferred_element_type=F32)
        else:
            block = jnp.concatenate([left, right], axis=1)
            half_width = left.shape[1]
            term = jnp.dot(hidden[...], block, preferred_element_type=F32)
        term = term.astype(BF16)
        pieces[i, 0] = term[:, :half_width]
        pieces[i, 1] = term[:, half_width:]
        for half, owner in enumerate(owners(i)):

            @pl.when(owner // per != tp)
            def _():
                f_copy(i, half, owner).start()

            @pl.when(owner // per == tp)
            def _():
                fin[tp, owner % per, half] = pieces[i, half]

    for load in loads[2:]:
        load.wait()
    down_block(0, down[0, 0], down[0, 1])

    def down_step(i, carry):
        @pl.when(i <= CHUNKS)
        def _():
            event(early + 1, i - 1)

        @pl.when(i > early + 1)
        def _():
            for c in range(CHUNKS):
                landed(i - 1, c)

                @pl.when(i < n - 1)
                def _():
                    for half in range(2):
                        d_copy(i, half, c, False).start()

        down_block(i, down[i, 0], down[i, 1])
        return carry

    lax.fori_loop(1, n, down_step, 0)

    for k in range(n_tp - 1):
        source = (tp + n_tp - 1 - k) % n_tp
        for o in range(per):
            for half in range(2):
                pltpu.make_async_remote_copy(
                    src_ref=pieces.at[0, half], dst_ref=fin.at[source, o, half],
                    send_sem=fsend.at[0, half], recv_sem=frecv.at[source, o, half],
                    device_id=(sp, peers[k]), device_id_type=MESH,
                ).wait_recv()
    piece = fin.shape[4]
    for o in range(per):
        for half in range(2):
            start = (2 * o + half) * piece
            total = own_stream[:, start:start + piece]
            mixed = fin[0, o, half].astype(F32)
            for t in range(1, n_tp):
                mixed = mixed + fin[t, o, half].astype(F32)
            out_ref[:, start:start + piece] = (total + mixed).astype(BF16)

    def drain(i, carry):
        for c in range(CHUNKS):
            for half in range(2):
                d_copy(i, half, c, True).wait_send()
        return carry

    lax.fori_loop(0, n - 1, drain, 0)

    def drain_pieces(i, carry):
        for half, owner in enumerate(owners(i)):

            @pl.when(owner // per != tp)
            def _():
                f_copy(i, half, owner).wait_send()

        return carry

    lax.fori_loop(0, n, drain_pieces, 0)
    for k in range(n_tp - 1):
        p_copy(k).wait_send()
        q_copy(k).wait_send()
        y_copy(k).wait_send()


def vmem():
    return pl.BlockSpec(memory_space=pltpu.VMEM)


def hbm():
    return pl.BlockSpec(memory_space=pl.ANY)


def fused_kernel(
    n, n_tp, heads, scale, nope_ref, rope_ref, lat_ref, kr_ref, lat_gain, freq_ref, wk_in, wv_in,
    wo_ref, gain_ref, res_hbm, wu, wd,
    out_ref,
    q_ref, spin,
    wk_ref, wv_ref, xs, keys_ref, vals_ref, peak, acc, res_ref,
    far32, stream_ref, sbuf, sin, xbuf, xgot, mine, sq_mine, sqs, ys, up, down, hidden,
    hold, pieces, xin, finh, finz,
    zx_send, yx_send, x_recv, share_send, share_recv,
    wz_send, wy_send, wb_send, w_recv, b_recv, own_sem,
    s_send, s_recv, r_send, r_recv, y_send, y_recv, q_send, q_recv, f_send, f_recv,
    c_send, c_recv, e_send, e_recv, res_sem,
):
    sp = lax.axis_index("sp")
    tp = lax.axis_index("tp")
    nz = n // 2
    z, y = sp // 2, sp % 2
    x_at, core = tp // 2, tp % 2
    sib = tp + 1 - 2 * core
    far = (tp + 2) % n_tp
    across = sp + 1 - 2 * y
    mate = 2 * (z + 1 - 2 * (z % 2)) + y
    turn = 1 - 2 * (z % 2)
    inner = (z > 0) & (z < nz - 1)
    peers = [(tp + k) % n_tp for k in range(1, n_tp)]

    def half_of(zz):
        return ((zz + 1) // 2) % 2

    def z_at(k):
        return (z + turn * k + nz) % nz

    barrier = pltpu.get_barrier_semaphore()
    greet = [(2 * ((z + k) % nz) + y, tp) for k in range(1, nz)]
    greet += [(across, tp)] + [(sp, p) for p in peers] + [(mate, p) for p in peers]
    for target in greet:
        pl.semaphore_signal(barrier, inc=1, device_id=target, device_id_type=MESH)
    pl.semaphore_wait(barrier, len(greet))

    def remote(src, dst, send, recv, target):
        return pltpu.make_async_remote_copy(
            src_ref=src, dst_ref=dst, send_sem=send, recv_sem=recv,
            device_id=target, device_id_type=MESH)

    latent = wk_ref.shape[1]
    value_width = wv_ref.shape[0] // heads
    rows = nope_ref.shape[0]
    half = rows // 2
    width = stream_ref.shape[1]
    depth = wu.shape[0]
    units = up.shape[2]
    cut_u, cut_d = depth // CUTS, units // CUTS
    share_w = wd.shape[1]

    def span(r):
        return pl.ds(r * half, half)

    def zx_copy(k):
        return remote(xs.at[sp, tp], xs.at[sp, tp], zx_send.at[k - 1], x_recv.at[sp],
                      (2 * z_at(k) + y, tp))

    def yx_copy(s):
        return remote(xs.at[s, tp], xs.at[s, tp],
                      yx_send.at[s], x_recv.at[s], (across, tp))

    def x_landed(s):
        remote(xs.at[s, tp], xs.at[s, tp], yx_send.at[s], x_recv.at[s], (across, tp)).wait_recv()

    def share(s, k):
        return remote(xs.at[s, tp], xs.at[s, tp], share_send.at[s, k], share_recv.at[s, tp],
                      (sp, peers[k]))

    def share_all(s):
        for k in range(n_tp - 1):
            share(s, k).start()

    def share_wait(s):
        for k in range(n_tp - 1):
            remote(xs.at[s, tp], xs.at[s, peers[k]], share_send.at[s, k],
                   share_recv.at[s, peers[k]], (sp, peers[k])).wait_recv()

    def w_src(m, c, h):
        if m == 0:
            return wu.at[pl.ds(c * cut_u, cut_u), pl.ds(pl.multiple_of(h * units, LANES), units)]
        return wd.at[pl.ds(h * units + c * cut_d, cut_d)]

    def w_slot(m, side, s, c):
        if m == 0:
            return up.at[side, pl.ds(s * depth + c * cut_u, cut_u)]
        return down.at[s, pl.ds(side * units + c * cut_d, cut_d)]

    def wz_copy(m, k, c):
        there = z_at(k)
        return remote(w_src(m, c, half_of(there)), w_slot(m, core, sp, c),
                      wz_send.at[m, k - 1, c], w_recv.at[m, sp, c], (2 * there + y, tp))

    def wy_copy(m, s, c, first):
        slot = w_slot(m, core, s, c)
        return remote(w_src(m, c, half_of(z)) if first else slot, slot,
                      wy_send.at[m, s, c], w_recv.at[m, s, c], (across, tp))

    def wb_copy(m, s, c, first):
        slot = w_slot(m, core, s, c)
        return remote(w_src(m, c, half_of(z)) if first else slot, slot,
                      wb_send.at[m, s, c], b_recv.at[m, s, c], (sp, sib))

    def w_landed(m, s, c):
        slot = w_slot(m, core, s, c)
        remote(slot, slot, wy_send.at[m, s, c], w_recv.at[m, s, c], (across, tp)).wait_recv()

    def b_landed(m, s):
        for c in range(CUTS):
            slot = w_slot(m, 1 - core, s, c)
            remote(slot, slot, wb_send.at[m, s, c], b_recv.at[m, s, c], (sp, sib)).wait_recv()

    def own_copy(m):
        h = half_of(z)
        if m == 0:
            src = wu.at[:, pl.ds(pl.multiple_of(h * units, LANES), units)]
            dst = up.at[core, pl.ds(sp * depth, depth)]
        else:
            src = wd.at[pl.ds(h * units, units)]
            dst = down.at[sp, pl.ds(core * units, units)]
        return pltpu.make_async_copy(src, dst, own_sem.at[m])

    def z_send(m, k):
        for c in range(CUTS):
            wz_copy(m, k, c).start()

    def late_sends(k, c0, c1):
        @pl.when(z * (nz - 1 - z) == 0)
        def _():
            for c in range(c0, c1):
                wz_copy(1, k, c).start()

    def step_of(i):
        return i + 1

    def from_z(m, i):
        s = 2 * z_at(step_of(i)) + y
        for c in range(CUTS):
            w_landed(m, s, c)
            wy_copy(m, s, c, False).start()
            wb_copy(m, s, c, False).start()

    def from_y(m, s):
        for c in range(CUTS):
            w_landed(m, s, c)
            wb_copy(m, s, c, False).start()

    def y_origin(i):
        return 2 * z_at(step_of(i)) + 1 - y

    def grid_of(shape):
        return (lax.broadcasted_iota(jnp.int32, shape, 0),
                lax.broadcasted_iota(jnp.int32, shape, 1))

    def picks(hit):
        return jnp.where(hit, 1.0, 0.0).astype(BF16)

    turn_half = ROPE // 2

    def turned(u, span_of):
        i, j = grid_of((span_of, span_of))
        swap = picks((i // ROPE == j // ROPE) & ((i + turn_half) % ROPE == j % ROPE))
        other = jnp.dot(u, swap, preferred_element_type=F32)
        return (u.astype(F32) * spin[0, :, :span_of] + other * spin[1, :, :span_of]).astype(BF16)

    def place(out, plain, rotated):
        i, j = grid_of((heads * UNROTATED_WIDTH, heads * LANES))
        first = picks((i // UNROTATED_WIDTH == j // LANES) & (i % UNROTATED_WIDTH == j % LANES))
        i, j = grid_of((heads * ROPE, heads * LANES))
        second = picks((i // ROPE == j // LANES) & (i % ROPE + UNROTATED_WIDTH == j % LANES))
        out[...] = (
            jnp.dot(plain[...], first, preferred_element_type=F32)
            + jnp.dot(rotated, second, preferred_element_type=F32)).astype(BF16)

    def flipped(u):
        i, j = grid_of((u.shape[1], u.shape[1]))
        return lax.dot_general(picks(i == j), u, NT, preferred_element_type=F32).astype(BF16)


    @pl.when(inner)
    def _():
        wz_copy(0, 2, 0).start()

    line, lane = grid_of((rows, LANES))
    phases = (sp * rows + line).astype(F32) * freq_ref[...]
    spin[0] = jnp.cos(phases)
    sine = jnp.sin(phases)
    spin[1] = jnp.where(lane % ROPE < turn_half, -sine, sine)
    lat = flipped(rms_scale(lat_ref[...].astype(F32), lat_gain[...]).astype(BF16))
    i, j = grid_of((ROPE, ROPE))
    keys = lax.dot_general(
        kr_ref[...], picks(i == j), (((0,), (0,)), ((), ())), preferred_element_type=F32)
    rot = flipped(turned(keys.astype(BF16), ROPE))
    chunk = rows // n_tp
    for t in range(n_tp):
        xs[sp, t, :latent] = lat[:, t * chunk:(t + 1) * chunk]
        xs[sp, t, latent:] = rot[:, t * chunk:(t + 1) * chunk]

    for k in range(1, nz):
        zx_copy(k).start()
    yx_copy(sp).start()
    for c in range(0, CUTS):
        wz_copy(0, 1, c).start()

    @pl.when(z * (nz - 1 - z) == 0)
    def _():
        wz_copy(0, 2, 0).start()

    for c in range(1, CUTS):
        wz_copy(0, 2, c).start()
    for k in range(3, nz):
        z_send(0, k)

    @pl.when(inner)
    def _():
        for k in range(1, nz):
            z_send(1, k)

    late_sends(1, 0, CUTS)
    for c in range(CUTS):
        wy_copy(0, sp, c, True).start()
    for m in range(2):
        own_copy(m).start()
    for m in range(2):
        for c in range(CUTS):
            wb_copy(m, sp, c, True).start()
    res_copy = pltpu.make_async_copy(
        res_hbm.at[:, pl.ds(pl.multiple_of(tp * width, LANES), width)], res_ref, res_sem)
    res_copy.start()
    wk_ref[...] = jnp.transpose(wk_in[...].astype(F32)).astype(BF16)
    wv_ref[...] = jnp.transpose(wv_in[...].astype(F32)).astype(BF16)
    peak[...] = jnp.full(peak.shape, -1e30, F32)
    acc[...] = jnp.zeros(acc.shape, F32)
    place(q_ref, nope_ref, turned(rope_ref[...], LANES))

    def project_keys(s):
        block = jnp.concatenate([xs[s, t] for t in range(n_tp)], axis=1)
        lat = block[:latent]
        rot = block[latent:]
        count = block.shape[1]
        k_all = jnp.dot(wk_ref[...], lat, preferred_element_type=F32).astype(BF16)
        v_all = jnp.dot(wv_ref[...], lat, preferred_element_type=F32).astype(BF16)
        k_pad = jnp.zeros((LANES - UNROTATED_WIDTH - rot.shape[0], count), BF16)
        ones = jnp.ones((16, count), BF16)
        v_pad = jnp.zeros((LANES - value_width - 16, count), BF16)
        for h in range(heads):
            keys_ref[s, h] = jnp.concatenate(
                [k_all[h * UNROTATED_WIDTH:(h + 1) * UNROTATED_WIDTH], rot, k_pad], axis=0)
            vals_ref[s, h] = jnp.concatenate(
                [v_all[h * value_width:(h + 1) * value_width], ones, v_pad], axis=0)

    def attend(s, r, size):
        lines = pl.ds(r * half, size)
        for h in range(heads):
            score = jnp.dot(q_ref[lines, h * LANES:(h + 1) * LANES], keys_ref[s, h],
                            preferred_element_type=F32)
            old = peak[h, lines]
            new = jnp.maximum(old, jnp.max(score, axis=1, keepdims=True))
            p = jnp.exp2((score - new) * scale).astype(BF16)
            acc[h, lines] = acc[h, lines] * jnp.exp2((old - new) * scale) + lax.dot_general(
                p, vals_ref[s, h], NT, preferred_element_type=F32)
            peak[h, lines] = new

    def block_at(b):
        flip = (b - 2) // (nz - 1)
        off = (b - 2) % (nz - 1) + 1
        there = 2 * ((z + off) % nz) + (y + flip) % 2
        return there

    def s_copy(r):
        return remote(sbuf.at[r], sin.at[r], s_send.at[r], s_recv.at[r], (sp, sib))

    def r_copy(r):
        return remote(xbuf.at[r], xgot.at[r], r_send.at[r], r_recv.at[r], (sp, far))

    def project(r):
        group = []
        for h in range(heads):
            a = acc[h, span(r)]
            group.append((a[:, :value_width] / a[:, value_width:value_width + 1]).astype(BF16))
        attended = jnp.concatenate(group, axis=1)

        def quarter(t):
            return jnp.dot(attended, wo_ref[:, pl.ds(pl.multiple_of(t * width, LANES), width)],
                           preferred_element_type=F32)

        sbuf[r, 0] = quarter(sib).astype(BF16)
        sbuf[r, 1] = quarter((sib + 2) % n_tp).astype(BF16)
        s_copy(r).start()
        far32[span(r)] = quarter(far)
        stream_ref[span(r)] = quarter(tp)

    def relay(r):
        s_copy(r).wait_recv()
        xbuf[r] = (far32[span(r)] + sin[r, 1].astype(F32)).astype(BF16)
        r_copy(r).start()

    home_far = 2 * (1 - x_at)

    def columns(t):
        return pl.ds(pl.multiple_of(t * width, LANES), width)

    def y_copy(r, which):
        target = ((sp, sib), (sp, home_far), (mate, 2 * x_at + 1))[which]
        return remote(mine.at[span(r)], ys.at[span(r), columns(tp)],
                      y_send.at[r, which], y_recv.at[r, tp], target)

    def q_copy(r, which):
        target = ((sp, sib), (sp, home_far), (mate, 2 * x_at + 1), (mate, home_far + 1))[which]
        return remote(sq_mine.at[r], sqs.at[r, tp], q_send.at[r, which], q_recv.at[r, tp], target)

    def f_copy(r, i):
        t = 2 * x_at + i
        return remote(ys.at[span(r), columns(t)], ys.at[span(r), columns(t)],
                      f_send.at[r, i], y_recv.at[r, t], (sp, home_far + 1))

    def y_wait(r, t):
        remote(mine.at[span(r)], ys.at[span(r), columns(t)],
               y_send.at[r, 1], y_recv.at[r, t], (sp, home_far)).wait_recv()

    def q_wait(r, t):
        remote(sq_mine.at[r], sqs.at[r, t], q_send.at[r, 1], q_recv.at[r, t],
               (sp, home_far)).wait_recv()

    def settle(r):
        r_copy(r).wait_recv()
        stream = stream_ref[span(r)] + sin[r, 0].astype(F32) + xgot[r].astype(F32)
        stream = stream + res_ref[span(r)].astype(F32)
        stream_ref[span(r)] = stream
        shard = (stream * gain_ref[tp]).astype(BF16)
        mine[span(r)] = shard
        total = jnp.sum(stream * stream, axis=1, keepdims=True)
        squares = jnp.transpose(jnp.broadcast_to(total, (half, LANES)))[:8]
        sq_mine[r] = squares

        @pl.when(core == 0)
        def _():
            ys[span(r), columns(tp)] = shard
            sqs[r, tp] = squares

        q_copy(r, 2).start()
        y_copy(r, 2).start()
        q_copy(r, 3).start()
        q_copy(r, 1).start()
        y_copy(r, 1).start()

        @pl.when(core == 1)
        def _():
            q_copy(r, 0).start()
            y_copy(r, 0).start()

    def pass_on(r):
        @pl.when(core == 1)
        def _():
            for i in range(2):
                y_wait(r, 2 * x_at + i)
                f_copy(r, i).start()

    def gathered(r):
        @pl.when(core == 1)
        def _():
            for i in range(2):
                y_wait(r, home_far + i)
            for t in range(n_tp):
                q_wait(r, t)

        @pl.when(core == 0)
        def _():
            for t in peers:
                y_wait(r, t)
                q_wait(r, t)

    project_keys(sp)
    attend(sp, 0, half)
    x_landed(across)
    share_all(across)
    attend(sp, 1, half)
    for off in range(1, nz):
        s = 2 * ((z + off) % nz) + y
        x_landed(s)
        yx_copy(s).start()
        share_all(s)
    for c in range(CUTS):
        wy_copy(1, sp, c, True).start()

    split = n // 2

    def first_blocks(b, carry):
        s = jnp.where(b == 1, across, block_at(b))
        share_wait(s)
        project_keys(s)
        attend(s, 0, rows)

        @pl.when(b == 2)
        def _():
            for off in range(1, nz):
                there = 2 * ((z + off) % nz) + 1 - y
                x_landed(there)
                share_all(there)
            from_z(0, 0)

        return carry

    def second_blocks(b, carry):
        s = block_at(b)
        share_wait(s)
        project_keys(s)
        attend(s, 0, half)

        @pl.when(b == n - 1)
        def _():
            from_y(0, across)
            from_z(0, 1)

        return carry

    def third_blocks(b, carry):
        attend(block_at(b), 1, half)

        @pl.when(b == split)
        def _():
            relay(0)

        @pl.when(b == split + 1)
        def _():
            from_y(0, y_origin(0))

        return carry

    lax.fori_loop(1, split, first_blocks, 0)
    lax.fori_loop(split, n, second_blocks, 0)
    res_copy.wait()
    project(0)
    lax.fori_loop(split, n, third_blocks, 0)
    project(1)
    settle(0)
    late_sends(2, 0, CUTS // 2)
    relay(1)
    for i in range(2, nz - 1):
        from_z(0, i)
    settle(1)
    late_sends(2, CUTS // 2, CUTS)
    late_sends(3, 0, CUTS)
    pass_on(0)
    from_y(0, y_origin(1))
    pass_on(1)
    for i in range(2, nz - 1):
        from_y(0, y_origin(i))
    from_z(1, 0)
    own_copy(0).wait()
    for s in range(n):
        b_landed(0, s)
    gathered(0)
    gathered(1)

    factors = []
    for r in range(2):
        squares = sqs[r, 0]
        for t in range(1, n_tp):
            squares = squares + sqs[r, t]
        squares = jnp.concatenate([squares] * (LANES // 8), axis=0)
        factors.append(jnp.transpose(squares)[:, :1])
    factor = lax.rsqrt(jnp.concatenate(factors, axis=0) / (width * n_tp) + epsilon)
    tile = math.gcd(units, 512)
    tiles = units // tile

    def up_step(i, carry):
        within = pl.ds(pl.multiple_of((i % tiles) * tile, tile), tile)
        total = jnp.dot(ys[...], up[i // tiles, :, within], preferred_element_type=F32)
        total = jnp.maximum(total, 0.0) * factor
        hidden[:, pl.ds(pl.multiple_of(i * tile, tile), tile)] = (total * total).astype(BF16)

        @pl.when(i == 1)
        def _():
            from_z(1, 1)

        return carry

    lax.fori_loop(0, 2 * tiles, up_step, 0)

    per = n // n_tp

    def order(j):
        i = (j - 2) // 2
        there = 2 * z_at(step_of(i)) + (y + j) % 2
        return jnp.where(j == 0, sp, jnp.where(j == 1, across, there))

    def c_copy(s, r):
        return remote(pieces.at[s, span(r)], xin.at[s % nz, span(r)], c_send.at[s, r],
                      c_recv.at[s % nz, r], (sp, far))

    def e_copy(s, r):
        return remote(pieces.at[s, span(r)], finh.at[s % per, span(r)], e_send.at[s, r],
                      e_recv.at[0, s % per, r], (sp, s // per))

    def g_copy(s, r):
        return remote(pieces.at[s, span(r)], finz.at[s % per, span(r)], e_send.at[s, r],
                      e_recv.at[1, s % per, r], (mate, s // per))

    def owner_is_here(s):
        return s // nz == x_at

    def finish(s):
        @pl.when(owner_is_here(s))
        def _():
            for r in range(2):
                c_copy(s, r).wait_recv()
                value = (hold[s % nz, span(r)] + xin[s % nz, span(r)].astype(F32)).astype(BF16)

                @pl.when((core == 0) & (s // per == tp))
                def _():
                    finh[s % per, span(r)] = value

                @pl.when((core == 1) | (s // per != tp))
                def _():
                    pieces[s, span(r)] = value

                    @pl.when(core == 1)
                    def _():
                        g_copy(s, r).start()

                    @pl.when(core == 0)
                    def _():
                        e_copy(s, r).start()

    own_copy(1).wait()

    def down_step(j, carry):
        s = order(j)
        i = (j - 2) // 2

        @pl.when(j % 2 == 1)
        def _():
            from_y(1, s)

        @pl.when((j % 2 == 0) & (j >= 4) & (j < n - 2))
        def _():
            from_z(1, i + 1)

        b_landed(1, s)
        term = jnp.dot(hidden[...], down[s], preferred_element_type=F32)

        @pl.when(owner_is_here(s))
        def _():
            hold[s % nz] = term

        @pl.when(s // nz != x_at)
        def _():
            pieces[s] = term.astype(BF16)
            for r in range(2):
                c_copy(s, r).start()

        @pl.when(j >= LAG)
        def _():
            finish(order(j - LAG))

        return carry

    lax.fori_loop(0, n, down_step, 0)

    def last_step(j, carry):
        finish(order(j))
        return carry

    lax.fori_loop(n - LAG, n, last_step, 0)

    for o in range(per):
        s = tp * per + o
        cols = slice(o * share_w, (o + 1) * share_w)
        for r in range(2):
            g_copy(s, r).wait_recv()

            @pl.when(core == 1)
            def _():
                e_copy(s, r).wait_recv()

            out_ref[span(r), cols] = (
                stream_ref[span(r), cols]
                + (finh[o, span(r)].astype(F32) + finz[o, span(r)].astype(F32))).astype(BF16)

    for k in range(1, nz):
        zx_copy(k).wait_send()
        for m in range(2):
            for c in range(CUTS):
                wz_copy(m, k, c).wait_send()
    yx_copy(sp).wait_send()
    for k in range(n_tp - 1):
        share(across, k).wait_send()
    for off in range(1, nz):
        s = 2 * ((z + off) % nz) + y
        yx_copy(s).wait_send()
        for k in range(n_tp - 1):
            share(s, k).wait_send()
            share(2 * ((z + off) % nz) + 1 - y, k).wait_send()
    for off in range(nz):
        s = 2 * ((z + off) % nz) + y
        for m in range(2):
            for c in range(CUTS):
                wy_copy(m, s, c, False).wait_send()

    def drain(s, carry):
        for m in range(2):
            for c in range(CUTS):
                wb_copy(m, s, c, False).wait_send()

        @pl.when(s // nz != x_at)
        def _():
            for r in range(2):
                c_copy(s, r).wait_send()

        @pl.when(owner_is_here(s) & ((core == 1) | (s // per != tp)))
        def _():
            for r in range(2):
                g_copy(s, r).wait_send()

        return carry

    lax.fori_loop(0, n, drain, 0)
    for r in range(2):
        s_copy(r).wait_send()
        r_copy(r).wait_send()
        for which in range(1, 3):
            y_copy(r, which).wait_send()
        for which in range(1, 4):
            q_copy(r, which).wait_send()

        @pl.when(core == 1)
        def _():
            y_copy(r, 0).wait_send()
            q_copy(r, 0).wait_send()
            for i in range(2):
                f_copy(r, i).wait_send()


def fused(
    n, n_tp, heads, scale, queries, rope_queries, latents, rope_keys, latent_gain,
    key_up, value_up, w_out, gain, residual, w_up, w_down,
):
    rows, model = residual.shape
    depth, units = w_up.shape[0], w_up.shape[1] // 2
    share_w = w_down.shape[1]
    width = model // n_tp
    wide = latents.shape[1] + ROPE
    rates = np.arange(0, ROPE, 2, dtype=np.float32) / np.float32(ROPE)
    rates = np.float32(1.0) / np.float32(rope_base) ** rates
    rates = np.tile(rates, LANES // rates.shape[0])[None, :]
    half, nz, per = rows // 2, n // 2, n // n_tp
    dma = pltpu.SemaphoreType.DMA
    return pl.pallas_call(
        functools.partial(fused_kernel, n, n_tp, heads, scale),
        out_shape=jax.ShapeDtypeStruct((rows, width), BF16),
        in_specs=[vmem()] * 10 + [hbm()] * 3,
        out_specs=vmem(),
        scratch_shapes=[
            pltpu.VMEM((rows, heads * LANES), BF16),
            pltpu.VMEM((2, rows, LANES), F32),
            pltpu.VMEM(key_up.shape[::-1], BF16),
            pltpu.VMEM(value_up.shape[::-1], BF16),
            pltpu.VMEM((n, n_tp, wide, rows // n_tp), BF16),
            pltpu.VMEM((n, heads, LANES, rows), BF16),
            pltpu.VMEM((n, heads, LANES, rows), BF16),
            pltpu.VMEM((heads, rows, 1), F32),
            pltpu.VMEM((heads, rows, LANES), F32),
            pltpu.VMEM((rows, width), BF16),
            pltpu.VMEM((rows, width), F32),
            pltpu.VMEM((rows, width), F32),
            pltpu.VMEM((2, 2, half, width), BF16),
            pltpu.VMEM((2, 2, half, width), BF16),
            pltpu.VMEM((2, half, width), BF16),
            pltpu.VMEM((2, half, width), BF16),
            pltpu.VMEM((rows, width), BF16),
            pltpu.VMEM((2, 8, half), F32),
            pltpu.VMEM((2, n_tp, 8, half), F32),
            pltpu.VMEM((rows, model), BF16),
            pltpu.VMEM((2, model, units), BF16),
            pltpu.VMEM((n, 2 * units, share_w), BF16),
            pltpu.VMEM((rows, 2 * units), BF16),
            pltpu.VMEM((nz, rows, share_w), F32),
            pltpu.VMEM((n, rows, share_w), BF16),
            pltpu.VMEM((nz, rows, share_w), BF16),
            pltpu.VMEM((per, rows, share_w), BF16),
            pltpu.VMEM((per, rows, share_w), BF16),
            dma((nz - 1,)), dma((n,)), dma((n,)), dma((n, n_tp - 1)), dma((n, n_tp)),
            dma((2, nz - 1, CUTS)), dma((2, n, CUTS)), dma((2, n, CUTS)),
            dma((2, n, CUTS)), dma((2, n, CUTS)), dma((2,)),
            dma((2,)), dma((2,)), dma((2,)), dma((2,)),
            dma((2, 3)), dma((2, n_tp)), dma((2, 4)), dma((2, n_tp)),
            dma((2, 2)), dma((2, 2)),
            dma((n, 2)), dma((nz, 2)), dma((n, 2)), dma((2, per, 2)), dma,
        ],
        compiler_params=pltpu.CompilerParams(
            collective_id=2, has_side_effects=True, vmem_limit_bytes=62 * 2**20),
        name="layer",
    )(
        queries, rope_queries, latents, jnp.transpose(rope_keys), latent_gain[None, :], jnp.asarray(rates),
        key_up, value_up, w_out, gain, residual, w_up, w_down,
    )


def on_device(
    n,
    n_tp,
    residual_in,
    queries_nope,
    queries_rope,
    latents,
    rope_keys,
    latent_norm_gain,
    key_up_weight,
    value_up_weight,
    w_out,
    norm_gain,
    w_up,
    w_down,
):
    rows, model = residual_in.shape
    heads = key_up_weight.shape[1] // UNROTATED_WIDTH
    value_width = value_up_weight.shape[1] // heads
    width = model // n_tp
    depth, units = w_up.shape
    scale = math.log2(math.e) / math.sqrt(UNROTATED_WIDTH + ROPE)
    lined = depth % (16 * CUTS) == 0 and w_down.shape[1] % LANES == 0 and rows % 512 == 0
    fits = heads * ROPE == LANES and n % 4 == 0 and n > 4 and n % (2 * n_tp) == 0
    if fits and lined and n_tp == 4:
        return fused(
            n, n_tp, heads, scale, queries_nope, queries_rope, latents, rope_keys,
            latent_norm_gain, key_up_weight, value_up_weight, w_out,
            norm_gain.reshape(n_tp, 1, width), residual_in, w_up, w_down)
    positions = lax.axis_index("sp") * rows + jnp.arange(rows, dtype=jnp.int32)
    phases = rope_phases(positions, ROPE)
    q_rot = rotate(
        queries_rope.astype(F32).reshape(rows, heads, ROPE), phases[:, None, :]
    ).astype(BF16)
    queries = jnp.concatenate(
        [
            queries_nope.reshape(rows, heads, UNROTATED_WIDTH),
            q_rot,
            jnp.zeros((rows, heads, LANES - UNROTATED_WIDTH - ROPE), BF16),
        ],
        axis=2,
    ).reshape(rows, heads * LANES)
    lat_norm = rms_scale(latents.astype(F32), latent_norm_gain).astype(BF16)
    key_rot = rotate(rope_keys.astype(F32), phases).astype(BF16)
    x = jnp.concatenate([lat_norm, key_rot], axis=1)
    wide = x.shape[1]
    x = jnp.transpose(x.reshape(n_tp, rows // n_tp, wide), (0, 2, 1))

    dma = pltpu.SemaphoreType.DMA
    part, full = pl.pallas_call(
        functools.partial(
            attention_kernel, n, n_tp, heads, scale),
        out_shape=(
            jax.ShapeDtypeStruct((n_tp, rows, width), BF16),
            jax.ShapeDtypeStruct((n, 2, CHUNKS, depth // 2 // CHUNKS, units), BF16),
        ),
        in_specs=[vmem()] * 5 + [hbm()],
        out_specs=(vmem(), hbm()),
        scratch_shapes=[
            pltpu.VMEM(key_up_weight.shape[::-1], BF16),
            pltpu.VMEM(value_up_weight.shape[::-1], BF16),
            pltpu.VMEM((n, n_tp, wide, rows // n_tp), BF16),
            pltpu.VMEM((heads, rows, 1), F32),
            pltpu.VMEM((heads, rows, LANES), F32),
            dma((n - 1,)), dma((n - 1,)),
            dma((n, n_tp - 1)), dma((n, n_tp - 1)),
            dma((n - 1, 2, CHUNKS)), dma((n - 1, 2, CHUNKS)), dma,
        ],
        compiler_params=pltpu.CompilerParams(
            collective_id=0, has_side_effects=True, vmem_limit_bytes=56 * 2**20),
        name="attend",
    )(
        queries, x, key_up_weight, value_up_weight,
        w_out, w_up.reshape(2, CHUNKS, depth // 2 // CHUNKS, units),
    )

    hidden_units, share = w_down.shape
    narrow = (share // 2) % LANES != 0
    if narrow:
        down_in = jnp.transpose(w_down.reshape(hidden_units, 2, share // 2), (1, 2, 0))
        half_shape = (share // 2, hidden_units)
    else:
        down_in = w_down
        half_shape = (hidden_units, share // 2)
    per = n // n_tp
    return pl.pallas_call(
        functools.partial(feed_kernel, n, n_tp, narrow),
        out_shape=jax.ShapeDtypeStruct((rows, width), BF16),
        in_specs=[vmem(), hbm(), vmem(), hbm(), hbm()],
        out_specs=vmem(),
        scratch_shapes=[
            pltpu.VMEM((rows, width), BF16),
            pltpu.VMEM((model, units), BF16),
            pltpu.VMEM((n, 2) + half_shape, BF16),
            pltpu.VMEM((n_tp - 1, rows, width), BF16),
            pltpu.VMEM((n_tp, rows, width), BF16),
            pltpu.VMEM((n_tp, 8, rows), F32),
            pltpu.VMEM((rows, width), F32),
            pltpu.VMEM((rows, units), BF16),
            pltpu.VMEM((n, 2, rows, share // 2), BF16),
            pltpu.VMEM((n_tp, per, 2, rows, share // 2), BF16),
            dma((n - 1, 2, CHUNKS)), dma((n - 1, 2, CHUNKS)),
            dma((n_tp - 1,)), dma((n_tp - 1,)),
            dma((n_tp - 1,)), dma((n_tp - 1,)),
            dma((n_tp - 1,)), dma((n_tp - 1,)),
            dma((n, 2)), dma((n_tp, per, 2)),
            dma((4,)),
        ],
        compiler_params=pltpu.CompilerParams(
            collective_id=1, has_side_effects=True, vmem_limit_bytes=60 * 2**20),
        name="feed",
    )(part, residual_in, norm_gain.reshape(n_tp, 1, width), full.reshape(model, units), down_in)


def solution(mesh):
    in_specs = (
        P("sp", None),
        P("sp", "tp"),
        P("sp", "tp"),
        P("sp", None),
        P("sp", None),
        P(),
        P(None, "tp"),
        P(None, "tp"),
        P("tp", None),
        P(),
        P("sp", "tp"),
        P("tp", "sp"),
    )
    out_specs = P("sp", "tp")
    return jax.shard_map(
        functools.partial(on_device, mesh.shape["sp"], mesh.shape["tp"]),
        mesh=mesh, in_specs=in_specs, out_specs=out_specs, check_vma=False,
    )
```

```python
import functools
import math

import jax
import jax.numpy as jnp
import numpy as np
from jax import lax
from jax.experimental import pallas as pl
from jax.experimental.pallas import tpu as pltpu
from jax.sharding import PartitionSpec as P

UNROTATED_WIDTH = 64
ROPE = 32
LANES = 128
CHUNKS = 4
CUTS = 2
LAG = 5

rope_base = 10000.0
epsilon = 1e-06
F32 = jnp.float32
BF16 = jnp.bfloat16
MESH = pl.DeviceIdType.MESH
NT = (((1,), (1,)), ((), ()))


def rotate(vectors, phases):
    half_width = vectors.shape[-1] // 2
    first_half = vectors[..., :half_width]
    second_half = vectors[..., half_width:]
    cosine = jnp.cos(phases)
    sine = jnp.sin(phases)
    return jnp.concatenate(
        [first_half * cosine - second_half * sine, second_half * cosine + first_half * sine],
        axis=-1,
    )


def rope_phases(positions, width):
    inverse = 1.0 / rope_base ** (jnp.arange(0, width, 2, dtype=jnp.float32) / width)
    return positions.astype(jnp.float32)[:, None] * inverse[None, :]


def rms_scale(vectors, gain_vec):
    return (
        vectors
        * lax.rsqrt(jnp.mean(vectors * vectors, axis=-1, keepdims=True) + epsilon)
        * gain_vec
    )


def ring_of(index, n):
    return index // 2 + (index % 2) * (n - 1 - 2 * (index // 2))


def index_of(place, n):
    return 2 * place + (place // (n // 2)) * (2 * n - 1 - 4 * place)


def ring_ids(n):
    place = ring_of(lax.axis_index("sp"), n)

    def at(offset):
        return index_of((place + offset + 2 * n) % n, n)

    return at


def attention_kernel(
    n, n_tp, heads, scale, q_ref, x_ref, wk_in, wv_in, wo_ref, wu_ref,
    part_ref, full_ref,
    wk_ref, wv_ref, xs, peak, acc, xsend, xrecv, ssend, srecv, wsend, wrecv, own_sem,
):
    at = ring_ids(n)
    tp = lax.axis_index("tp")
    me = lax.axis_index("sp")
    to = ((at(1), tp), (at(-1), tp))
    peers = [(tp + k) % n_tp for k in range(1, n_tp)]
    onward = (at(1 - 2 * (tp % 2)), tp)
    barrier = pltpu.get_barrier_semaphore()
    for target in list(to) + [(me, p) for p in peers]:
        pl.semaphore_signal(barrier, inc=1, device_id=target, device_id_type=MESH)
    pl.semaphore_wait(barrier, 2 + n_tp - 1)

    latent = wk_ref.shape[1]
    value_width = wv_ref.shape[0] // heads

    def x_copy(step, src):
        return pltpu.make_async_remote_copy(
            src_ref=src, dst_ref=xs.at[step + 1, tp],
            send_sem=xsend.at[step], recv_sem=xrecv.at[step],
            device_id=onward, device_id_type=MESH,
        )

    def share(step, k):
        return pltpu.make_async_remote_copy(
            src_ref=xs.at[step, tp], dst_ref=xs.at[step, tp],
            send_sem=ssend.at[step, k], recv_sem=srecv.at[step, k],
            device_id=(me, peers[k]), device_id_type=MESH,
        )

    def share_wait(step):
        for k in range(n_tp - 1):
            pltpu.make_async_remote_copy(
                src_ref=xs.at[step, tp], dst_ref=xs.at[step, (tp + n_tp - 1 - k) % n_tp],
                send_sem=ssend.at[step, k], recv_sem=srecv.at[step, k],
                device_id=(me, peers[k]), device_id_type=MESH,
            ).wait_recv()

    def w_copy(step, half, c, first):
        owner = at(-step) if half == 0 else at(step)
        return pltpu.make_async_remote_copy(
            src_ref=wu_ref.at[half, c] if first else full_ref.at[owner, half, c],
            dst_ref=full_ref.at[owner, half, c],
            send_sem=wsend.at[step, half, c], recv_sem=wrecv.at[step, half, c],
            device_id=to[half], device_id_type=MESH,
        )

    x_copy(0, x_ref.at[tp]).start()
    for c in range(CHUNKS):
        for half in range(2):
            w_copy(0, half, c, True).start()
    own = pltpu.make_async_copy(wu_ref, full_ref.at[me], own_sem)
    own.start()
    wk_ref[...] = jnp.transpose(wk_in[...].astype(F32)).astype(BF16)
    wv_ref[...] = jnp.transpose(wv_in[...].astype(F32)).astype(BF16)
    peak[...] = jnp.full(peak.shape, -1e30, F32)
    acc[...] = jnp.zeros(acc.shape, F32)

    def attend(blocks):
        block = jnp.concatenate(blocks, axis=1)
        lat = block[:latent]
        rot = block[latent:]
        keys = block.shape[1]
        k_all = jnp.dot(wk_ref[...], lat, preferred_element_type=F32).astype(BF16)
        v_all = jnp.dot(wv_ref[...], lat, preferred_element_type=F32).astype(BF16)
        k_pad = jnp.zeros((LANES - UNROTATED_WIDTH - rot.shape[0], keys), BF16)
        ones = jnp.ones((16, keys), BF16)
        v_pad = jnp.zeros((LANES - value_width - 16, keys), BF16)
        for h in range(heads):
            k_h = jnp.concatenate(
                [k_all[h * UNROTATED_WIDTH:(h + 1) * UNROTATED_WIDTH], rot, k_pad], axis=0)
            v_h = jnp.concatenate(
                [v_all[h * value_width:(h + 1) * value_width], ones, v_pad], axis=0)
            s = jnp.dot(q_ref[:, h * LANES:(h + 1) * LANES], k_h, preferred_element_type=F32)
            old = peak[h]
            new = jnp.maximum(old, jnp.max(s, axis=1, keepdims=True))
            p = jnp.exp2((s - new) * scale).astype(BF16)
            acc[h] = acc[h] * jnp.exp2((old - new) * scale) + lax.dot_general(
                p, v_h, NT, preferred_element_type=F32)
            peak[h] = new

    def turn(i, carry):
        x_copy(i - 1, x_ref.at[tp]).wait_recv()
        x_copy(i, xs.at[i, tp]).start()
        for k in range(n_tp - 1):
            share(i, k).start()
        for c in range(CHUNKS):
            for half in range(2):
                w_copy(i - 1, half, c, True).wait_recv()
                w_copy(i, half, c, False).start()

        @pl.when(i > 1)
        def _():
            share_wait(i - 1)
            attend([xs[i - 1, t] for t in range(n_tp)])

        return carry

    attend([x_ref[t] for t in range(n_tp)])
    lax.fori_loop(1, n - 1, turn, 0)
    x_copy(n - 2, x_ref.at[tp]).wait_recv()
    for k in range(n_tp - 1):
        share(n - 1, k).start()

    def last(i, carry):
        share_wait(i)
        attend([xs[i, t] for t in range(n_tp)])
        return carry

    lax.fori_loop(n - 2, n, last, 0)

    width = part_ref.shape[2]
    group = []
    for h in range(heads):
        a = acc[h]
        group.append((a[:, :value_width] / a[:, value_width:value_width + 1]).astype(BF16))
    attended = jnp.concatenate(group, axis=1)
    for j in range(part_ref.shape[0]):
        part_ref[j] = jnp.dot(
            attended, wo_ref[:, j * width:(j + 1) * width], preferred_element_type=F32
        ).astype(BF16)

    own.wait()
    for c in range(CHUNKS):
        for half in range(2):
            w_copy(n - 2, half, c, True).wait_recv()

    def drain(i, carry):
        x_copy(i, x_ref.at[tp]).wait_send()
        for k in range(n_tp - 1):
            share(i + 1, k).wait_send()
        for c in range(CHUNKS):
            for half in range(2):
                w_copy(i, half, c, True).wait_send()
        return carry

    lax.fori_loop(0, n - 1, drain, 0)


def feed_kernel(
    n, n_tp, narrow, part_ref, res_hbm, gain_ref, up_hbm, wd_hbm,
    out_ref,
    res_ref, up, down, parts, ys, sq, own_stream, hidden, pieces, fin,
    dsend, drecv, psend, precv, ysend, yrecv, qsend, qrecv, fsend, frecv, local,
):
    at = ring_ids(n)
    tp = lax.axis_index("tp")
    sp = lax.axis_index("sp")
    to = ((at(1), tp), (at(-1), tp))
    peers = [(tp + k) % n_tp for k in range(1, n_tp)]
    barrier = pltpu.get_barrier_semaphore()
    for target in list(to) + [(sp, p) for p in peers]:
        pl.semaphore_signal(barrier, inc=1, device_id=target, device_id_type=MESH)
    pl.semaphore_wait(barrier, 2 + n_tp - 1)

    rows, width = res_ref.shape
    per = n // n_tp

    lines = down.shape[2] // CHUNKS

    def own_half(half):
        if narrow:
            return wd_hbm.at[half]
        return wd_hbm.at[:, half * down.shape[3]:(half + 1) * down.shape[3]]

    def d_copy(step, half, c, first):
        span = pl.ds(c * lines, lines)
        if not first:
            src = down.at[step, half, span]
        elif narrow:
            src = wd_hbm.at[half, span]
        else:
            src = wd_hbm.at[span, half * down.shape[3]:(half + 1) * down.shape[3]]
        return pltpu.make_async_remote_copy(
            src_ref=src, dst_ref=down.at[step + 1, half, span],
            send_sem=dsend.at[step, half, c], recv_sem=drecv.at[step, half, c],
            device_id=to[half], device_id_type=MESH,
        )

    def p_copy(k):
        peer = peers[k]
        return pltpu.make_async_remote_copy(
            src_ref=part_ref.at[peer], dst_ref=parts.at[k],
            send_sem=psend.at[k], recv_sem=precv.at[k],
            device_id=(sp, peer), device_id_type=MESH,
        )

    def y_copy(k):
        return pltpu.make_async_remote_copy(
            src_ref=ys.at[tp], dst_ref=ys.at[tp],
            send_sem=ysend.at[k], recv_sem=yrecv.at[k],
            device_id=(sp, peers[k]), device_id_type=MESH,
        )

    def q_copy(k):
        return pltpu.make_async_remote_copy(
            src_ref=sq.at[0], dst_ref=sq.at[k + 1],
            send_sem=qsend.at[k], recv_sem=qrecv.at[k],
            device_id=(sp, peers[k]), device_id_type=MESH,
        )

    def landed(step, c):
        for half in range(2):
            d_copy(step, half, c, True).wait_recv()

    def event(step, c):
        landed(step - 1, c)
        for half in range(2):
            d_copy(step, half, c, False).start()

    def events(first, last):
        for tick in range(first, last):
            event(1 + tick // CHUNKS, tick % CHUNKS)

    for c in range(CHUNKS):
        for half in range(2):
            d_copy(0, half, c, True).start()
    for k in range(n_tp - 1):
        p_copy(k).start()
    loads = [
        pltpu.make_async_copy(
            res_hbm.at[:, pl.ds(pl.multiple_of(tp * width, LANES), width)], res_ref, local.at[0]),
        pltpu.make_async_copy(up_hbm, up, local.at[1]),
        pltpu.make_async_copy(own_half(0), down.at[0, 0], local.at[2]),
        pltpu.make_async_copy(own_half(1), down.at[0, 1], local.at[3]),
    ]
    for load in loads:
        load.start()

    early = 4
    events(0, 6)
    for k in range(n_tp - 1):
        p_copy(k).wait_recv()
    loads[0].wait()
    stream = part_ref[tp].astype(F32)
    for k in range(n_tp - 1):
        stream = stream + parts[k].astype(F32)
    stream = stream + res_ref[...].astype(F32)
    own_stream[...] = stream
    ys[tp] = (stream * gain_ref[tp]).astype(BF16)
    total = jnp.sum(stream * stream, axis=1, keepdims=True)
    sq[0] = jnp.transpose(jnp.broadcast_to(total, (rows, LANES)))[:8]
    for k in range(n_tp - 1):
        q_copy(k).start()
        y_copy(k).start()
    events(6, 12)
    for k in range(n_tp - 1):
        q_copy(k).wait_recv()
    for k in range(n_tp - 1):
        pltpu.make_async_remote_copy(
            src_ref=ys.at[tp], dst_ref=ys.at[(tp + n_tp - 1 - k) % n_tp],
            send_sem=ysend.at[k], recv_sem=yrecv.at[k],
            device_id=(sp, peers[k]), device_id_type=MESH,
        ).wait_recv()
    squares = sq[0]
    for k in range(1, n_tp):
        squares = squares + sq[k]
    squares = jnp.concatenate([squares] * (LANES // 8), axis=0)
    factor = lax.rsqrt(jnp.transpose(squares)[:, :1] / (width * n_tp) + epsilon)
    loads[1].wait()
    units = hidden.shape[1]
    tile = math.gcd(units, 512)

    def up_step(c, carry):
        columns = pl.ds(pl.multiple_of(c * tile, tile), tile)
        total = jnp.dot(ys[0], up[:width, columns], preferred_element_type=F32)
        for t in range(1, n_tp):
            total = total + jnp.dot(
                ys[t], up[t * width:(t + 1) * width, columns], preferred_element_type=F32)
        total = jnp.maximum(total, 0.0) * factor
        hidden[:, columns] = (total * total).astype(BF16)

        @pl.when(c < CHUNKS)
        def _():
            event(early, c)

        return carry

    lax.fori_loop(0, units // tile, up_step, 0)

    def owners(i):
        return at(-i), at(i)

    def f_copy(i, half, owner):
        return pltpu.make_async_remote_copy(
            src_ref=pieces.at[i, half],
            dst_ref=fin.at[tp, owner % per, half],
            send_sem=fsend.at[i, half], recv_sem=frecv.at[tp, owner % per, half],
            device_id=(sp, owner // per), device_id_type=MESH,
        )

    def down_block(i, left, right):
        if narrow:
            block = jnp.concatenate([left, right], axis=0)
            half_width = left.shape[0]
            term = lax.dot_general(hidden[...], block, NT, preferred_element_type=F32)
        else:
            block = jnp.concatenate([left, right], axis=1)
            half_width = left.shape[1]
            term = jnp.dot(hidden[...], block, preferred_element_type=F32)
        term = term.astype(BF16)
        pieces[i, 0] = term[:, :half_width]
        pieces[i, 1] = term[:, half_width:]
        for half, owner in enumerate(owners(i)):

            @pl.when(owner // per != tp)
            def _():
                f_copy(i, half, owner).start()

            @pl.when(owner // per == tp)
            def _():
                fin[tp, owner % per, half] = pieces[i, half]

    for load in loads[2:]:
        load.wait()
    down_block(0, down[0, 0], down[0, 1])

    def down_step(i, carry):
        @pl.when(i <= CHUNKS)
        def _():
            event(early + 1, i - 1)

        @pl.when(i > early + 1)
        def _():
            for c in range(CHUNKS):
                landed(i - 1, c)

                @pl.when(i < n - 1)
                def _():
                    for half in range(2):
                        d_copy(i, half, c, False).start()

        down_block(i, down[i, 0], down[i, 1])
        return carry

    lax.fori_loop(1, n, down_step, 0)

    for k in range(n_tp - 1):
        source = (tp + n_tp - 1 - k) % n_tp
        for o in range(per):
            for half in range(2):
                pltpu.make_async_remote_copy(
                    src_ref=pieces.at[0, half], dst_ref=fin.at[source, o, half],
                    send_sem=fsend.at[0, half], recv_sem=frecv.at[source, o, half],
                    device_id=(sp, peers[k]), device_id_type=MESH,
                ).wait_recv()
    piece = fin.shape[4]
    for o in range(per):
        for half in range(2):
            start = (2 * o + half) * piece
            total = own_stream[:, start:start + piece]
            mixed = fin[0, o, half].astype(F32)
            for t in range(1, n_tp):
                mixed = mixed + fin[t, o, half].astype(F32)
            out_ref[:, start:start + piece] = (total + mixed).astype(BF16)

    def drain(i, carry):
        for c in range(CHUNKS):
            for half in range(2):
                d_copy(i, half, c, True).wait_send()
        return carry

    lax.fori_loop(0, n - 1, drain, 0)

    def drain_pieces(i, carry):
        for half, owner in enumerate(owners(i)):

            @pl.when(owner // per != tp)
            def _():
                f_copy(i, half, owner).wait_send()

        return carry

    lax.fori_loop(0, n, drain_pieces, 0)
    for k in range(n_tp - 1):
        p_copy(k).wait_send()
        q_copy(k).wait_send()
        y_copy(k).wait_send()


def vmem():
    return pl.BlockSpec(memory_space=pltpu.VMEM)


def hbm():
    return pl.BlockSpec(memory_space=pl.ANY)


def fused_kernel(
    n, n_tp, heads, scale, nope_ref, rope_ref, lat_ref, kr_ref, lat_gain, freq_ref, wk_in, wv_in,
    wo_hbm, gain_ref, res_hbm, wu, wd,
    out_ref,
    wo_ref, wo_sem, q_ref, spin,
    wk_ref, wv_ref, xs, keys_ref, vals_ref, peak, acc, res_ref,
    far32, stream_ref, sbuf, sin, xbuf, xgot, mine, sq_mine, sqs, ys, up, down, hidden,
    hold, pieces, xin, finh, finz,
    zx_send, yx_send, x_recv, share_send, share_recv,
    wz_send, wy_send, wb_send, w_recv, b_recv, own_sem,
    s_send, s_recv, r_send, r_recv, y_send, y_recv, q_send, q_recv, f_send, f_recv,
    c_send, c_recv, e_send, e_recv, res_sem,
):
    sp = lax.axis_index("sp")
    tp = lax.axis_index("tp")
    nz = n // 2
    z, y = sp // 2, sp % 2
    x_at, core = tp // 2, tp % 2
    sib = tp + 1 - 2 * core
    far = (tp + 2) % n_tp
    across = sp + 1 - 2 * y
    mate = 2 * (z + 1 - 2 * (z % 2)) + y
    turn = 1 - 2 * (z % 2)
    inner = (z > 0) & (z < nz - 1)
    peers = [(tp + k) % n_tp for k in range(1, n_tp)]

    def half_of(zz):
        return ((zz + 1) // 2) % 2

    def z_at(k):
        return (z + turn * k + nz) % nz

    barrier = pltpu.get_barrier_semaphore()
    greet = [(2 * ((z + k) % nz) + y, tp) for k in range(1, nz)]
    greet += [(across, tp)] + [(sp, p) for p in peers] + [(mate, p) for p in peers]
    for target in greet:
        pl.semaphore_signal(barrier, inc=1, device_id=target, device_id_type=MESH)
    pl.semaphore_wait(barrier, len(greet))

    def remote(src, dst, send, recv, target):
        return pltpu.make_async_remote_copy(
            src_ref=src, dst_ref=dst, send_sem=send, recv_sem=recv,
            device_id=target, device_id_type=MESH)

    latent = wk_ref.shape[1]
    value_width = wv_ref.shape[0] // heads
    rows = nope_ref.shape[0]
    half = rows // 2
    width = stream_ref.shape[1]
    depth = wu.shape[0]
    units = up.shape[2]
    cut_u, cut_d = depth // CUTS, units // CUTS
    share_w = wd.shape[1]

    def span(r):
        return pl.ds(r * half, half)

    def zx_copy(k):
        return remote(xs.at[sp, tp], xs.at[sp, tp], zx_send.at[k - 1], x_recv.at[sp],
                      (2 * z_at(k) + y, tp))

    def yx_copy(s):
        return remote(xs.at[s, tp], xs.at[s, tp],
                      yx_send.at[s], x_recv.at[s], (across, tp))

    def x_landed(s):
        remote(xs.at[s, tp], xs.at[s, tp], yx_send.at[s], x_recv.at[s], (across, tp)).wait_recv()

    def share(s, k):
        return remote(xs.at[s, tp], xs.at[s, tp], share_send.at[s, k], share_recv.at[s, tp],
                      (sp, peers[k]))

    def share_all(s):
        for k in range(n_tp - 1):
            share(s, k).start()

    def share_wait(s):
        for k in range(n_tp - 1):
            remote(xs.at[s, tp], xs.at[s, peers[k]], share_send.at[s, k],
                   share_recv.at[s, peers[k]], (sp, peers[k])).wait_recv()

    def w_src(m, c, h):
        if m == 0:
            return wu.at[pl.ds(c * cut_u, cut_u), pl.ds(pl.multiple_of(h * units, LANES), units)]
        return wd.at[pl.ds(h * units + c * cut_d, cut_d)]

    def w_slot(m, side, s, c):
        if m == 0:
            return up.at[side, pl.ds(s * depth + c * cut_u, cut_u)]
        return down.at[s, pl.ds(side * units + c * cut_d, cut_d)]

    def wz_copy(m, k, c):
        there = z_at(k)
        return remote(w_src(m, c, half_of(there)), w_slot(m, core, sp, c),
                      wz_send.at[m, k - 1, c], w_recv.at[m, sp, c], (2 * there + y, tp))

    def wy_copy(m, s, c, first):
        slot = w_slot(m, core, s, c)
        return remote(w_src(m, c, half_of(z)) if first else slot, slot,
                      wy_send.at[m, s, c], w_recv.at[m, s, c], (across, tp))

    def wb_copy(m, s, c, first):
        slot = w_slot(m, core, s, c)
        return remote(w_src(m, c, half_of(z)) if first else slot, slot,
                      wb_send.at[m, s, c], b_recv.at[m, s, c], (sp, sib))

    def w_landed(m, s, c):
        slot = w_slot(m, core, s, c)
        remote(slot, slot, wy_send.at[m, s, c], w_recv.at[m, s, c], (across, tp)).wait_recv()

    def b_landed(m, s):
        for c in range(CUTS):
            slot = w_slot(m, 1 - core, s, c)
            remote(slot, slot, wb_send.at[m, s, c], b_recv.at[m, s, c], (sp, sib)).wait_recv()

    def own_copy(m):
        h = half_of(z)
        if m == 0:
            src = wu.at[:, pl.ds(pl.multiple_of(h * units, LANES), units)]
            dst = up.at[core, pl.ds(sp * depth, depth)]
        else:
            src = wd.at[pl.ds(h * units, units)]
            dst = down.at[sp, pl.ds(core * units, units)]
        return pltpu.make_async_copy(src, dst, own_sem.at[m])

    def z_send(m, k):
        for c in range(CUTS):
            wz_copy(m, k, c).start()

    def late_sends(k, c0, c1):
        @pl.when(z * (nz - 1 - z) == 0)
        def _():
            for c in range(c0, c1):
                wz_copy(1, k, c).start()

    def step_of(i):
        return i + 1

    def from_z(m, i):
        s = 2 * z_at(step_of(i)) + y
        for c in range(CUTS):
            w_landed(m, s, c)
            wy_copy(m, s, c, False).start()
            wb_copy(m, s, c, False).start()

    def from_y(m, s):
        for c in range(CUTS):
            w_landed(m, s, c)
            wb_copy(m, s, c, False).start()

    def y_origin(i):
        return 2 * z_at(step_of(i)) + 1 - y

    def grid_of(shape):
        return (lax.broadcasted_iota(jnp.int32, shape, 0),
                lax.broadcasted_iota(jnp.int32, shape, 1))

    def picks(hit):
        return jnp.where(hit, 1.0, 0.0).astype(BF16)

    turn_half = ROPE // 2

    def turned(u, span_of):
        i, j = grid_of((span_of, span_of))
        swap = picks((i // ROPE == j // ROPE) & ((i + turn_half) % ROPE == j % ROPE))
        other = jnp.dot(u, swap, preferred_element_type=F32)
        return (u.astype(F32) * spin[0, :, :span_of] + other * spin[1, :, :span_of]).astype(BF16)

    def place(out, plain, rotated):
        i, j = grid_of((heads * UNROTATED_WIDTH, heads * LANES))
        first = picks((i // UNROTATED_WIDTH == j // LANES) & (i % UNROTATED_WIDTH == j % LANES))
        i, j = grid_of((heads * ROPE, heads * LANES))
        second = picks((i // ROPE == j // LANES) & (i % ROPE + UNROTATED_WIDTH == j % LANES))
        out[...] = (
            jnp.dot(plain[...], first, preferred_element_type=F32)
            + jnp.dot(rotated, second, preferred_element_type=F32)).astype(BF16)

    def flipped(u):
        i, j = grid_of((u.shape[1], u.shape[1]))
        return lax.dot_general(picks(i == j), u, NT, preferred_element_type=F32).astype(BF16)


    @pl.when(inner)
    def _():
        wz_copy(0, 2, 0).start()

    line, lane = grid_of((rows, LANES))
    phases = (sp * rows + line).astype(F32) * freq_ref[...]
    spin[0] = jnp.cos(phases)
    sine = jnp.sin(phases)
    spin[1] = jnp.where(lane % ROPE < turn_half, -sine, sine)
    lat = flipped(rms_scale(lat_ref[...].astype(F32), lat_gain[...]).astype(BF16))
    i, j = grid_of((ROPE, ROPE))
    keys = lax.dot_general(
        kr_ref[...], picks(i == j), (((0,), (0,)), ((), ())), preferred_element_type=F32)
    rot = flipped(turned(keys.astype(BF16), ROPE))
    chunk = rows // n_tp
    for t in range(n_tp):
        xs[sp, t, :latent] = lat[:, t * chunk:(t + 1) * chunk]
        xs[sp, t, latent:] = rot[:, t * chunk:(t + 1) * chunk]

    for k in range(1, nz):
        zx_copy(k).start()
    yx_copy(sp).start()
    for c in range(0, CUTS):
        wz_copy(0, 1, c).start()

    @pl.when(z * (nz - 1 - z) == 0)
    def _():
        wz_copy(0, 2, 0).start()

    for c in range(1, CUTS):
        wz_copy(0, 2, c).start()
    for k in range(3, nz):
        z_send(0, k)

    @pl.when(inner)
    def _():
        for k in range(1, nz):
            z_send(1, k)

    late_sends(1, 0, CUTS)
    for c in range(CUTS):
        wy_copy(0, sp, c, True).start()
    for m in range(2):
        own_copy(m).start()
    for m in range(2):
        for c in range(CUTS):
            wb_copy(m, sp, c, True).start()
    res_copy = pltpu.make_async_copy(
        res_hbm.at[:, pl.ds(pl.multiple_of(tp * width, LANES), width)], res_ref, res_sem)
    res_copy.start()
    wo_copy = pltpu.make_async_copy(wo_hbm, wo_ref, wo_sem)
    wo_copy.start()
    wk_ref[...] = jnp.transpose(wk_in[...].astype(F32)).astype(BF16)
    wv_ref[...] = jnp.transpose(wv_in[...].astype(F32)).astype(BF16)
    peak[...] = jnp.full(peak.shape, -1e30, F32)
    acc[...] = jnp.zeros(acc.shape, F32)
    place(q_ref, nope_ref, turned(rope_ref[...], LANES))

    def project_keys(s):
        block = jnp.concatenate([xs[s, t] for t in range(n_tp)], axis=1)
        lat = block[:latent]
        rot = block[latent:]
        count = block.shape[1]
        k_all = jnp.dot(wk_ref[...], lat, preferred_element_type=F32).astype(BF16)
        v_all = jnp.dot(wv_ref[...], lat, preferred_element_type=F32).astype(BF16)
        k_pad = jnp.zeros((LANES - UNROTATED_WIDTH - rot.shape[0], count), BF16)
        ones = jnp.ones((16, count), BF16)
        v_pad = jnp.zeros((LANES - value_width - 16, count), BF16)
        for h in range(heads):
            keys_ref[s, h] = jnp.concatenate(
                [k_all[h * UNROTATED_WIDTH:(h + 1) * UNROTATED_WIDTH], rot, k_pad], axis=0)
            vals_ref[s, h] = jnp.concatenate(
                [v_all[h * value_width:(h + 1) * value_width], ones, v_pad], axis=0)

    def attend(s, r, size):
        lines = pl.ds(r * half, size)
        for h in range(heads):
            score = jnp.dot(q_ref[lines, h * LANES:(h + 1) * LANES], keys_ref[s, h],
                            preferred_element_type=F32)
            old = peak[h, lines]
            new = jnp.maximum(old, jnp.max(score, axis=1, keepdims=True))
            p = jnp.exp2((score - new) * scale).astype(BF16)
            acc[h, lines] = acc[h, lines] * jnp.exp2((old - new) * scale) + lax.dot_general(
                p, vals_ref[s, h], NT, preferred_element_type=F32)
            peak[h, lines] = new

    def block_at(b):
        flip = (b - 2) // (nz - 1)
        off = (b - 2) % (nz - 1) + 1
        there = 2 * ((z + off) % nz) + (y + flip) % 2
        return there

    def s_copy(r):
        return remote(sbuf.at[r], sin.at[r], s_send.at[r], s_recv.at[r], (sp, sib))

    def r_copy(r):
        return remote(xbuf.at[r], xgot.at[r], r_send.at[r], r_recv.at[r], (sp, far))

    def project(r):
        group = []
        for h in range(heads):
            a = acc[h, span(r)]
            group.append((a[:, :value_width] / a[:, value_width:value_width + 1]).astype(BF16))
        attended = jnp.concatenate(group, axis=1)

        def quarter(t):
            return jnp.dot(attended, wo_ref[:, pl.ds(pl.multiple_of(t * width, LANES), width)],
                           preferred_element_type=F32)

        sbuf[r, 0] = quarter(sib).astype(BF16)
        sbuf[r, 1] = quarter((sib + 2) % n_tp).astype(BF16)
        s_copy(r).start()
        far32[span(r)] = quarter(far)
        stream_ref[span(r)] = quarter(tp)

    def relay(r):
        s_copy(r).wait_recv()
        xbuf[r] = (far32[span(r)] + sin[r, 1].astype(F32)).astype(BF16)
        r_copy(r).start()

    home_far = 2 * (1 - x_at)

    def columns(t):
        return pl.ds(pl.multiple_of(t * width, LANES), width)

    def y_copy(r, which):
        target = ((sp, sib), (sp, home_far), (mate, 2 * x_at + 1))[which]
        return remote(mine.at[span(r)], ys.at[span(r), columns(tp)],
                      y_send.at[r, which], y_recv.at[r, tp], target)

    def q_copy(r, which):
        target = ((sp, sib), (sp, home_far), (mate, 2 * x_at + 1), (mate, home_far + 1))[which]
        return remote(sq_mine.at[r], sqs.at[r, tp], q_send.at[r, which], q_recv.at[r, tp], target)

    def f_copy(r, i):
        t = 2 * x_at + i
        return remote(ys.at[span(r), columns(t)], ys.at[span(r), columns(t)],
                      f_send.at[r, i], y_recv.at[r, t], (sp, home_far + 1))

    def y_wait(r, t):
        remote(mine.at[span(r)], ys.at[span(r), columns(t)],
               y_send.at[r, 1], y_recv.at[r, t], (sp, home_far)).wait_recv()

    def q_wait(r, t):
        remote(sq_mine.at[r], sqs.at[r, t], q_send.at[r, 1], q_recv.at[r, t],
               (sp, home_far)).wait_recv()

    def settle(r):
        r_copy(r).wait_recv()
        stream = stream_ref[span(r)] + sin[r, 0].astype(F32) + xgot[r].astype(F32)
        stream = stream + res_ref[span(r)].astype(F32)
        stream_ref[span(r)] = stream
        shard = (stream * gain_ref[tp]).astype(BF16)
        mine[span(r)] = shard
        total = jnp.sum(stream * stream, axis=1, keepdims=True)
        squares = jnp.transpose(jnp.broadcast_to(total, (half, LANES)))[:8]
        sq_mine[r] = squares

        @pl.when(core == 0)
        def _():
            ys[span(r), columns(tp)] = shard
            sqs[r, tp] = squares

        q_copy(r, 2).start()
        y_copy(r, 2).start()
        q_copy(r, 3).start()
        q_copy(r, 1).start()
        y_copy(r, 1).start()

        @pl.when(core == 1)
        def _():
            q_copy(r, 0).start()
            y_copy(r, 0).start()

    def pass_on(r):
        @pl.when(core == 1)
        def _():
            for i in range(2):
                y_wait(r, 2 * x_at + i)
                f_copy(r, i).start()

    def gathered(r):
        @pl.when(core == 1)
        def _():
            for i in range(2):
                y_wait(r, home_far + i)
            for t in range(n_tp):
                q_wait(r, t)

        @pl.when(core == 0)
        def _():
            for t in peers:
                y_wait(r, t)
                q_wait(r, t)

    project_keys(sp)
    attend(sp, 0, half)
    x_landed(across)
    share_all(across)
    attend(sp, 1, half)
    for off in range(1, nz):
        s = 2 * ((z + off) % nz) + y
        x_landed(s)
        yx_copy(s).start()
        share_all(s)
    for c in range(CUTS):
        wy_copy(1, sp, c, True).start()

    split = n // 2

    def first_blocks(b, carry):
        s = jnp.where(b == 1, across, block_at(b))
        share_wait(s)
        project_keys(s)
        attend(s, 0, rows)

        @pl.when(b == 2)
        def _():
            for off in range(1, nz):
                there = 2 * ((z + off) % nz) + 1 - y
                x_landed(there)
                share_all(there)
            from_z(0, 0)

        return carry

    def second_blocks(b, carry):
        s = block_at(b)
        share_wait(s)
        project_keys(s)
        attend(s, 0, half)

        @pl.when(b == n - 1)
        def _():
            from_y(0, across)
            from_z(0, 1)

        return carry

    def third_blocks(b, carry):
        attend(block_at(b), 1, half)

        @pl.when(b == split)
        def _():
            relay(0)

        @pl.when(b == split + 1)
        def _():
            from_y(0, y_origin(0))

        return carry

    lax.fori_loop(1, split, first_blocks, 0)
    lax.fori_loop(split, n, second_blocks, 0)
    res_copy.wait()
    wo_copy.wait()
    project(0)
    lax.fori_loop(split, n, third_blocks, 0)
    project(1)
    settle(0)
    late_sends(2, 0, CUTS // 2)
    relay(1)
    for i in range(2, nz - 1):
        from_z(0, i)
    settle(1)
    late_sends(2, CUTS // 2, CUTS)
    late_sends(3, 0, CUTS)
    pass_on(0)
    for i in range(1, nz - 1):
        from_y(0, y_origin(i))
    from_z(1, 0)
    pass_on(1)
    own_copy(0).wait()
    for s in range(n):
        b_landed(0, s)
    gathered(0)
    gathered(1)

    factors = []
    for r in range(2):
        squares = sqs[r, 0]
        for t in range(1, n_tp):
            squares = squares + sqs[r, t]
        squares = jnp.concatenate([squares] * (LANES // 8), axis=0)
        factors.append(jnp.transpose(squares)[:, :1])
    factor = lax.rsqrt(jnp.concatenate(factors, axis=0) / (width * n_tp) + epsilon)
    tile = math.gcd(units, 512)
    tiles = units // tile

    def up_step(i, carry):
        within = pl.ds(pl.multiple_of((i % tiles) * tile, tile), tile)
        total = jnp.dot(ys[...], up[i // tiles, :, within], preferred_element_type=F32)
        total = jnp.maximum(total, 0.0) * factor
        hidden[:, pl.ds(pl.multiple_of(i * tile, tile), tile)] = (total * total).astype(BF16)

        @pl.when(i == 1)
        def _():
            from_z(1, 1)

        return carry

    lax.fori_loop(0, 2 * tiles, up_step, 0)

    per = n // n_tp

    def order(j):
        i = (j - 2) // 2
        there = 2 * z_at(step_of(i)) + (y + j) % 2
        return jnp.where(j == 0, sp, jnp.where(j == 1, across, there))

    def c_copy(s, r):
        return remote(pieces.at[s, span(r)], xin.at[s % nz, span(r)], c_send.at[s, r],
                      c_recv.at[s % nz, r], (sp, far))

    def e_copy(s, r):
        return remote(pieces.at[s, span(r)], finh.at[s % per, span(r)], e_send.at[s, r],
                      e_recv.at[0, s % per, r], (sp, s // per))

    def g_copy(s, r):
        return remote(pieces.at[s, span(r)], finz.at[s % per, span(r)], e_send.at[s, r],
                      e_recv.at[1, s % per, r], (mate, s // per))

    def owner_is_here(s):
        return s // nz == x_at

    def finish(s):
        @pl.when(owner_is_here(s))
        def _():
            for r in range(2):
                c_copy(s, r).wait_recv()
                value = (hold[s % nz, span(r)] + xin[s % nz, span(r)].astype(F32)).astype(BF16)

                @pl.when((core == 0) & (s // per == tp))
                def _():
                    finh[s % per, span(r)] = value

                @pl.when((core == 1) | (s // per != tp))
                def _():
                    pieces[s, span(r)] = value

                    @pl.when(core == 1)
                    def _():
                        g_copy(s, r).start()

                    @pl.when(core == 0)
                    def _():
                        e_copy(s, r).start()

    own_copy(1).wait()

    def down_step(j, carry):
        s = order(j)
        i = (j - 2) // 2

        @pl.when(j % 2 == 1)
        def _():
            from_y(1, s)

        @pl.when((j % 2 == 0) & (j >= 4) & (j < n - 2))
        def _():
            from_z(1, i + 1)

        b_landed(1, s)
        term = jnp.dot(hidden[...], down[s], preferred_element_type=F32)

        @pl.when(owner_is_here(s))
        def _():
            hold[s % nz] = term

        @pl.when(s // nz != x_at)
        def _():
            pieces[s] = term.astype(BF16)
            for r in range(2):
                c_copy(s, r).start()

        @pl.when(j >= LAG)
        def _():
            finish(order(j - LAG))

        return carry

    lax.fori_loop(0, n, down_step, 0)

    def last_step(j, carry):
        finish(order(j))
        return carry

    lax.fori_loop(n - LAG, n, last_step, 0)

    for o in range(per):
        s = tp * per + o
        cols = slice(o * share_w, (o + 1) * share_w)
        for r in range(2):
            g_copy(s, r).wait_recv()

            @pl.when(core == 1)
            def _():
                e_copy(s, r).wait_recv()

            out_ref[span(r), cols] = (
                stream_ref[span(r), cols]
                + (finh[o, span(r)].astype(F32) + finz[o, span(r)].astype(F32))).astype(BF16)

    for k in range(1, nz):
        zx_copy(k).wait_send()
        for m in range(2):
            for c in range(CUTS):
                wz_copy(m, k, c).wait_send()
    yx_copy(sp).wait_send()
    for k in range(n_tp - 1):
        share(across, k).wait_send()
    for off in range(1, nz):
        s = 2 * ((z + off) % nz) + y
        yx_copy(s).wait_send()
        for k in range(n_tp - 1):
            share(s, k).wait_send()
            share(2 * ((z + off) % nz) + 1 - y, k).wait_send()
    for off in range(nz):
        s = 2 * ((z + off) % nz) + y
        for m in range(2):
            for c in range(CUTS):
                wy_copy(m, s, c, False).wait_send()

    def drain(s, carry):
        for m in range(2):
            for c in range(CUTS):
                wb_copy(m, s, c, False).wait_send()

        @pl.when(s // nz != x_at)
        def _():
            for r in range(2):
                c_copy(s, r).wait_send()

        @pl.when(owner_is_here(s) & ((core == 1) | (s // per != tp)))
        def _():
            for r in range(2):
                g_copy(s, r).wait_send()

        return carry

    lax.fori_loop(0, n, drain, 0)
    for r in range(2):
        s_copy(r).wait_send()
        r_copy(r).wait_send()
        for which in range(1, 3):
            y_copy(r, which).wait_send()
        for which in range(1, 4):
            q_copy(r, which).wait_send()

        @pl.when(core == 1)
        def _():
            y_copy(r, 0).wait_send()
            q_copy(r, 0).wait_send()
            for i in range(2):
                f_copy(r, i).wait_send()


def fused(
    n, n_tp, heads, scale, queries, rope_queries, latents, rope_keys, latent_gain,
    key_up, value_up, w_out, gain, residual, w_up, w_down,
):
    rows, model = residual.shape
    depth, units = w_up.shape[0], w_up.shape[1] // 2
    share_w = w_down.shape[1]
    width = model // n_tp
    wide = latents.shape[1] + ROPE
    rates = np.arange(0, ROPE, 2, dtype=np.float32) / np.float32(ROPE)
    rates = np.float32(1.0) / np.float32(rope_base) ** rates
    rates = np.tile(rates, LANES // rates.shape[0])[None, :]
    half, nz, per = rows // 2, n // 2, n // n_tp
    dma = pltpu.SemaphoreType.DMA
    return pl.pallas_call(
        functools.partial(fused_kernel, n, n_tp, heads, scale),
        out_shape=jax.ShapeDtypeStruct((rows, width), BF16),
        in_specs=[vmem()] * 8 + [hbm(), vmem()] + [hbm()] * 3,
        out_specs=vmem(),
        scratch_shapes=[
            pltpu.VMEM(w_out.shape, BF16), dma,
            pltpu.VMEM((rows, heads * LANES), BF16),
            pltpu.VMEM((2, rows, LANES), F32),
            pltpu.VMEM(key_up.shape[::-1], BF16),
            pltpu.VMEM(value_up.shape[::-1], BF16),
            pltpu.VMEM((n, n_tp, wide, rows // n_tp), BF16),
            pltpu.VMEM((n, heads, LANES, rows), BF16),
            pltpu.VMEM((n, heads, LANES, rows), BF16),
            pltpu.VMEM((heads, rows, 1), F32),
            pltpu.VMEM((heads, rows, LANES), F32),
            pltpu.VMEM((rows, width), BF16),
            pltpu.VMEM((rows, width), F32),
            pltpu.VMEM((rows, width), F32),
            pltpu.VMEM((2, 2, half, width), BF16),
            pltpu.VMEM((2, 2, half, width), BF16),
            pltpu.VMEM((2, half, width), BF16),
            pltpu.VMEM((2, half, width), BF16),
            pltpu.VMEM((rows, width), BF16),
            pltpu.VMEM((2, 8, half), F32),
            pltpu.VMEM((2, n_tp, 8, half), F32),
            pltpu.VMEM((rows, model), BF16),
            pltpu.VMEM((2, model, units), BF16),
            pltpu.VMEM((n, 2 * units, share_w), BF16),
            pltpu.VMEM((rows, 2 * units), BF16),
            pltpu.VMEM((nz, rows, share_w), F32),
            pltpu.VMEM((n, rows, share_w), BF16),
            pltpu.VMEM((nz, rows, share_w), BF16),
            pltpu.VMEM((per, rows, share_w), BF16),
            pltpu.VMEM((per, rows, share_w), BF16),
            dma((nz - 1,)), dma((n,)), dma((n,)), dma((n, n_tp - 1)), dma((n, n_tp)),
            dma((2, nz - 1, CUTS)), dma((2, n, CUTS)), dma((2, n, CUTS)),
            dma((2, n, CUTS)), dma((2, n, CUTS)), dma((2,)),
            dma((2,)), dma((2,)), dma((2,)), dma((2,)),
            dma((2, 3)), dma((2, n_tp)), dma((2, 4)), dma((2, n_tp)),
            dma((2, 2)), dma((2, 2)),
            dma((n, 2)), dma((nz, 2)), dma((n, 2)), dma((2, per, 2)), dma,
        ],
        compiler_params=pltpu.CompilerParams(
            collective_id=2, has_side_effects=True, vmem_limit_bytes=62 * 2**20),
        name="layer",
    )(
        queries, rope_queries, latents, jnp.transpose(rope_keys), latent_gain[None, :], jnp.asarray(rates),
        key_up, value_up, w_out, gain, residual, w_up, w_down,
    )


def on_device(
    n,
    n_tp,
    residual_in,
    queries_nope,
    queries_rope,
    latents,
    rope_keys,
    latent_norm_gain,
    key_up_weight,
    value_up_weight,
    w_out,
    norm_gain,
    w_up,
    w_down,
):
    rows, model = residual_in.shape
    heads = key_up_weight.shape[1] // UNROTATED_WIDTH
    value_width = value_up_weight.shape[1] // heads
    width = model // n_tp
    depth, units = w_up.shape
    scale = math.log2(math.e) / math.sqrt(UNROTATED_WIDTH + ROPE)
    lined = depth % (16 * CUTS) == 0 and w_down.shape[1] % LANES == 0 and rows % 512 == 0
    fits = heads * ROPE == LANES and n % 4 == 0 and n > 4 and n % (2 * n_tp) == 0
    if fits and lined and n_tp == 4:
        return fused(
            n, n_tp, heads, scale, queries_nope, queries_rope, latents, rope_keys,
            latent_norm_gain, key_up_weight, value_up_weight, w_out,
            norm_gain.reshape(n_tp, 1, width), residual_in, w_up, w_down)
    positions = lax.axis_index("sp") * rows + jnp.arange(rows, dtype=jnp.int32)
    phases = rope_phases(positions, ROPE)
    q_rot = rotate(
        queries_rope.astype(F32).reshape(rows, heads, ROPE), phases[:, None, :]
    ).astype(BF16)
    queries = jnp.concatenate(
        [
            queries_nope.reshape(rows, heads, UNROTATED_WIDTH),
            q_rot,
            jnp.zeros((rows, heads, LANES - UNROTATED_WIDTH - ROPE), BF16),
        ],
        axis=2,
    ).reshape(rows, heads * LANES)
    lat_norm = rms_scale(latents.astype(F32), latent_norm_gain).astype(BF16)
    key_rot = rotate(rope_keys.astype(F32), phases).astype(BF16)
    x = jnp.concatenate([lat_norm, key_rot], axis=1)
    wide = x.shape[1]
    x = jnp.transpose(x.reshape(n_tp, rows // n_tp, wide), (0, 2, 1))

    dma = pltpu.SemaphoreType.DMA
    part, full = pl.pallas_call(
        functools.partial(
            attention_kernel, n, n_tp, heads, scale),
        out_shape=(
            jax.ShapeDtypeStruct((n_tp, rows, width), BF16),
            jax.ShapeDtypeStruct((n, 2, CHUNKS, depth // 2 // CHUNKS, units), BF16),
        ),
        in_specs=[vmem()] * 5 + [hbm()],
        out_specs=(vmem(), hbm()),
        scratch_shapes=[
            pltpu.VMEM(key_up_weight.shape[::-1], BF16),
            pltpu.VMEM(value_up_weight.shape[::-1], BF16),
            pltpu.VMEM((n, n_tp, wide, rows // n_tp), BF16),
            pltpu.VMEM((heads, rows, 1), F32),
            pltpu.VMEM((heads, rows, LANES), F32),
            dma((n - 1,)), dma((n - 1,)),
            dma((n, n_tp - 1)), dma((n, n_tp - 1)),
            dma((n - 1, 2, CHUNKS)), dma((n - 1, 2, CHUNKS)), dma,
        ],
        compiler_params=pltpu.CompilerParams(
            collective_id=0, has_side_effects=True, vmem_limit_bytes=56 * 2**20),
        name="attend",
    )(
        queries, x, key_up_weight, value_up_weight,
        w_out, w_up.reshape(2, CHUNKS, depth // 2 // CHUNKS, units),
    )

    hidden_units, share = w_down.shape
    narrow = (share // 2) % LANES != 0
    if narrow:
        down_in = jnp.transpose(w_down.reshape(hidden_units, 2, share // 2), (1, 2, 0))
        half_shape = (share // 2, hidden_units)
    else:
        down_in = w_down
        half_shape = (hidden_units, share // 2)
    per = n // n_tp
    return pl.pallas_call(
        functools.partial(feed_kernel, n, n_tp, narrow),
        out_shape=jax.ShapeDtypeStruct((rows, width), BF16),
        in_specs=[vmem(), hbm(), vmem(), hbm(), hbm()],
        out_specs=vmem(),
        scratch_shapes=[
            pltpu.VMEM((rows, width), BF16),
            pltpu.VMEM((model, units), BF16),
            pltpu.VMEM((n, 2) + half_shape, BF16),
            pltpu.VMEM((n_tp - 1, rows, width), BF16),
            pltpu.VMEM((n_tp, rows, width), BF16),
            pltpu.VMEM((n_tp, 8, rows), F32),
            pltpu.VMEM((rows, width), F32),
            pltpu.VMEM((rows, units), BF16),
            pltpu.VMEM((n, 2, rows, share // 2), BF16),
            pltpu.VMEM((n_tp, per, 2, rows, share // 2), BF16),
            dma((n - 1, 2, CHUNKS)), dma((n - 1, 2, CHUNKS)),
            dma((n_tp - 1,)), dma((n_tp - 1,)),
            dma((n_tp - 1,)), dma((n_tp - 1,)),
            dma((n_tp - 1,)), dma((n_tp - 1,)),
            dma((n, 2)), dma((n_tp, per, 2)),
            dma((4,)),
        ],
        compiler_params=pltpu.CompilerParams(
            collective_id=1, has_side_effects=True, vmem_limit_bytes=60 * 2**20),
        name="feed",
    )(part, residual_in, norm_gain.reshape(n_tp, 1, width), full.reshape(model, units), down_in)


def solution(mesh):
    in_specs = (
        P("sp", None),
        P("sp", "tp"),
        P("sp", "tp"),
        P("sp", None),
        P("sp", None),
        P(),
        P(None, "tp"),
        P(None, "tp"),
        P("tp", None),
        P(),
        P("sp", "tp"),
        P("tp", "sp"),
    )
    out_specs = P("sp", "tp")
    return jax.shard_map(
        functools.partial(on_device, mesh.shape["sp"], mesh.shape["tp"]),
        mesh=mesh, in_specs=in_specs, out_specs=out_specs, check_vma=False,
    )
```
